128 devices in a mesh: sp: 64 (over z, y, x), tp: 2 (over core).
Axes of the slice: x: 4, y: 4, z: 4, core: 2. Of those that a mesh axis runs over, the one named last changes fastest.
Arguments:
- tokens: bfloat16 [32768, 4096], P(('sp', 'tp')), may hold values from -6 to 6
- norm_gain: float32 [4096], replicated, may hold values from 0.5 to 1.5
- query_weight: bfloat16 [4096, 1024], P(None, 'tp'), may hold values from -0.09375 to 0.09375
- key_weight: bfloat16 [4096, 1024], P(None, 'tp'), may hold values from -0.09375 to 0.09375
- value_weight: bfloat16 [4096, 2048], P(None, 'tp'), may hold values from -0.09375 to 0.09375
- gate_weight: bfloat16 [4096, 2048], P(None, 'tp'), may hold values from -0.09375 to 0.09375
- decay_bias: float32 [1024], P('tp'), may hold values from -0.5 to 0.5
- head_gain: float32 [2048], P('tp'), may hold values from 0.5 to 1.5
- out_weight: bfloat16 [2048, 4096], P('tp'), may hold values from -0.125 to 0.125
Outputs:
- layer_out: bfloat16 [32768, 4096], P(('sp', 'tp'))
The draws below stay inside these ranges and needn't reach their ends.
All inputs are finite; a program needn't handle non-finite values.
Results may differ from the reference program's by a relative error of at most 0.015.
Values may be sent and summed in bfloat16 or wider, within the bound.
A program may use at most 192 MiB of HBM per device.

```python
import math
import jax
import jax.numpy as jnp
from jax import lax

D = 4096
HEADS = 8
HEAD_K = 128
HEAD_V = 256
BLOCK = 64
SEQ = 32768
KEY_DIM = 1024
VALUE_DIM = 2048


def level_of(own_key, dims, cuts, least, top_value):
    level, own = 1.0, jax.random.fold_in(own_key, 6)
    for axis_at, shards_of in cuts:
        steps = jnp.exp(jax.random.uniform(jax.random.fold_in(own, axis_at), (shards_of,), jnp.float32, least / len(cuts), top_value / len(cuts)))
        level = level * jnp.repeat(steps, dims[axis_at] // shards_of).reshape([-1 if axis == axis_at else 1 for axis in range(len(dims))])
    return level


def bell_draw(rng, extent, spread, reach, shards=(), kind=jnp.bfloat16):
    gain = level_of(rng, extent, shards, -0.22, 0.18) if shards else 1.0
    array = jax.random.normal(rng, extent, jnp.float32) * spread * gain
    return jnp.minimum(jnp.maximum(array, -reach), reach).astype(kind)


def setup_inputs(seed: int = 0) -> dict:
    key_list = jax.random.split(jax.random.key(seed), 10)
    tokens = bell_draw(key_list[0], (SEQ, D), 1.0, 6.0, ((0, 128),))
    norm_gain = jnp.clip(1.0 + 0.1 * jax.random.normal(key_list[1], (D,), jnp.float32), 0.5, 1.5)
    query_weight = bell_draw(key_list[2], (D, KEY_DIM), D ** -0.5, 0.09375, ((1, 2),))
    key_weight = bell_draw(key_list[3], (D, KEY_DIM), D ** -0.5, 0.09375, ((1, 2),))
    value_weight = bell_draw(key_list[4], (D, VALUE_DIM), D ** -0.5, 0.09375, ((1, 2),))
    gate_weight = bell_draw(key_list[5], (D, VALUE_DIM), D ** -0.5, 0.09375, ((1, 2),))
    decay_bias = jnp.clip(jax.random.uniform(key_list[6], (KEY_DIM,), jnp.float32, -0.5, 0.5) * level_of(key_list[6], (KEY_DIM,), ((0, 2),), -0.4, 0.0), -0.5, 0.5)
    head_gain = jnp.clip(1.0 + 0.1 * jax.random.normal(key_list[7], (VALUE_DIM,), jnp.float32), 0.5, 1.5)
    out_weight = bell_draw(key_list[8], (VALUE_DIM, D), VALUE_DIM ** -0.5, 0.125, ((0, 2),))
    return {"tokens": tokens, "norm_gain": norm_gain, "query_weight": query_weight, "key_weight": key_weight, "value_weight": value_weight, "gate_weight": gate_weight, "decay_bias": decay_bias, "head_gain": head_gain, "out_weight": out_weight}


epsilon = 1e-06
decay_power = 16.0
precise = lax.Precision.HIGHEST

def to_blocks(values, head_count, head_width):
    block_count = values.shape[0] // BLOCK
    return values.astype(jnp.float32).reshape(block_count, BLOCK, head_count, head_width).transpose(0, 2, 1, 3)

def reference(tokens, norm_gain, query_weight, key_weight, value_weight, gate_weight, decay_bias, head_gain, out_weight):
    inputs = tokens.astype(jnp.float32)
    row_scale = lax.rsqrt(lax.optimization_barrier(jnp.mean(inputs * inputs, axis=-1, keepdims=True)) + epsilon)
    normed = (inputs * row_scale * norm_gain.astype(jnp.float32)).astype(jnp.bfloat16)
    query_rows = jnp.dot(normed, query_weight, preferred_element_type=jnp.float32).astype(jnp.bfloat16)
    key_rows = jnp.dot(normed, key_weight, preferred_element_type=jnp.float32).astype(jnp.bfloat16)
    value_rows = jnp.dot(normed, value_weight, preferred_element_type=jnp.float32).astype(jnp.bfloat16)
    gate_input = jnp.dot(normed, gate_weight, preferred_element_type=jnp.float32).astype(jnp.bfloat16)
    logits = decay_bias.astype(jnp.float32) + math.log(SEQ / 8.0)
    log_decay = jnp.broadcast_to(jax.nn.log_sigmoid(logits) / decay_power, (SEQ, KEY_DIM))
    query_blocks = to_blocks(query_rows, HEADS, HEAD_K) * HEAD_K ** (-0.5)
    key_blocks = to_blocks(key_rows, HEADS, HEAD_K)
    value_blocks = to_blocks(value_rows, HEADS, HEAD_V)
    decay_blocks = to_blocks(log_decay, HEADS, HEAD_K)
    within = jnp.cumsum(decay_blocks, axis=2)
    block_end = within[:, :, -1:, :]
    query_in = query_blocks * jnp.exp(within)
    key_in = key_blocks * jnp.exp(-within)
    key_out = key_blocks * jnp.exp(block_end - within)
    causal = jnp.tril(jnp.ones((BLOCK, BLOCK), dtype=bool))
    scores = jnp.where(causal, jnp.einsum('nhid,nhjd->nhij', query_in, key_in, precision=precise), 0.0)
    local_out = jnp.einsum('nhij,nhjv->nhiv', scores, value_blocks, precision=precise)
    block_decay = jnp.exp(block_end[:, :, 0, :])

    def advance(carry_state, inputs_now):
        query_now, key_now, value_now, decay_now = inputs_now
        carried = jnp.einsum('hid,hdv->hiv', query_now, carry_state, precision=precise)
        carry_state = decay_now[..., None] * carry_state + jnp.einsum('hjd,hjv->hdv', key_now, value_now, precision=precise)
        return (carry_state, carried)
    start_state = jnp.zeros((HEADS, HEAD_K, HEAD_V), jnp.float32)
    _, carried_out = lax.scan(advance, start_state, (query_in, key_out, value_blocks, block_decay))
    mixed_heads = (local_out + carried_out).transpose(0, 2, 1, 3).reshape(SEQ, HEADS, HEAD_V)
    head_scale = lax.rsqrt(lax.optimization_barrier(jnp.mean(mixed_heads * mixed_heads, axis=-1, keepdims=True)) + epsilon)
    normed_heads = (mixed_heads * head_scale * head_gain.astype(jnp.float32).reshape(HEADS, HEAD_V)).reshape(SEQ, HEADS * HEAD_V)
    gated_rows = (normed_heads * jax.nn.silu(gate_input.astype(jnp.float32))).astype(jnp.bfloat16)
    return jnp.dot(gated_rows, out_weight, preferred_element_type=jnp.float32).astype(jnp.bfloat16)
```

```python
import functools
import math

import jax
import jax.numpy as jnp
from jax import lax
from jax.experimental import pallas as pl
from jax.experimental.pallas import tpu as pltpu
from jax.sharding import Mesh
from jax.sharding import PartitionSpec as P

HEAD_K = 128
HEAD_V = 256
Z, Y, X, TP = "sp_0", "sp_1", "sp_2", "tp"
SP_TP = (Z, Y, X, TP)
MESH = pl.DeviceIdType.MESH
UNIT = 512
EPS = 1e-06
DECAY_POWER = 16.0
F32, BF16 = jnp.float32, jnp.bfloat16


def remote(src, dst, send, recv, where):
    return pltpu.make_async_remote_copy(
        src_ref=src, dst_ref=dst, send_sem=send, recv_sem=recv, device_id=where, device_id_type=MESH
    )


def dot(a, b, dims=((1,), (0,))):
    return lax.dot_general(a, b, (dims, ((), ())), preferred_element_type=F32)


def mixer(
    sizes,
    tok, gain, wq, wk, wv, wg, bias, hgain, wo,
    out,
    xn, wkb, wvb, wqb, wgb, wob, wpb, gainb, biasb, hgainb,
    kb, qb, vb, gsb, lob, sb, acc, ost,
    sa, ra, tb, rb, yp, tc, rc, dd, pd,
    gown, gsnd, grcv,
    tok_sem, w_sem, small_sem, wo_sem, out_sem,
    xs, xr, ps, pr, gs_s, gs_r, scan_s, scan_r,
):
    nz, ny, nx = sizes
    rows, width = xn.shape[1], xn.shape[2]
    heads = kb.shape[1]
    pairs = heads // 2
    chunk = HEAD_K // nx
    token_steps = tok_sem.shape[0]
    step_rows = rows // token_steps
    vsteps, osteps = wvb.shape[0], wob.shape[0]
    z, y, x, c = (lax.axis_index(a) for a in SP_TP)
    other = 1 - c
    chip = (z * ny + y) * nx + x
    seq = nz * ny * nx * 2 * rows

    def token_copy(i):
        r = pl.ds(i * step_rows, step_rows)
        return pltpu.make_async_copy(tok.at[r, :], xn.at[c, r, :], tok_sem.at[i])

    small = [(gain, gainb), (bias, biasb), (hgain, hgainb)]
    small = [pltpu.make_async_copy(a, b, small_sem.at[i]) for i, (a, b) in enumerate(small)]
    cols = lambda n: pl.ds(n * UNIT, UNIT)
    wk_copy = pltpu.make_async_copy(wk, wkb, w_sem.at[0])
    wq_copy = pltpu.make_async_copy(wq, wqb, w_sem.at[1])
    wv_copy = [pltpu.make_async_copy(wv.at[:, cols(n)], wvb.at[n], w_sem.at[2 + n]) for n in range(vsteps)]
    wg_copy = [pltpu.make_async_copy(wg.at[:, cols(n)], wgb.at[n], w_sem.at[2 + vsteps + n]) for n in range(vsteps)]
    wo_copy = [pltpu.make_async_copy(wo.at[:, cols(n)], wob.at[n], wo_sem.at[n]) for n in range(osteps)]
    for i in range(token_steps):
        token_copy(i).start()
    for s in small:
        s.start()
    for s in [wk_copy, *wv_copy, wq_copy, *wg_copy, *wo_copy]:
        s.start()

    barrier = pltpu.get_barrier_semaphore()
    peers = [{TP: other}]
    peers += [{X: lax.rem(x + d, nx)} for d in range(1, nx)]
    peers += [{Y: lax.rem(y + d, ny)} for d in range(1, ny)]
    peers += [{Z: lax.rem(z + d, nz)} for d in range(1, nz)]
    for peer in peers:
        pl.semaphore_signal(barrier, inc=1, device_id=peer, device_id_type=MESH)

    def x_send(i):
        r = pl.ds(i * step_rows, step_rows)
        return remote(xn.at[c, r, :], xn.at[c, r, :], xs.at[i], xr.at[i], {TP: other})

    def x_recv(i):
        r = pl.ds(i * step_rows, step_rows)
        return remote(xn.at[other, r, :], xn.at[other, r, :], xs.at[i], xr.at[i], {TP: other})

    for s in small:
        s.wait()
    for i in range(token_steps):
        token_copy(i).wait()

        @pl.loop(0, step_rows // 16)
        def _(g):
            r = pl.ds(pl.multiple_of(i * step_rows + g * 16, 16), 16)
            v = xn[c, r, :].astype(F32)
            scale = lax.rsqrt(jnp.mean(v * v, axis=-1, keepdims=True) + EPS)
            v = xn[c, r, :].astype(F32)
            xn[c, r, :] = (v * scale * gainb[...]).astype(BF16)

        if i == 0:
            pl.semaphore_wait(barrier, len(peers))
        x_send(i).start()

    logits = biasb[...] + math.log(seq / 8.0)
    log_decay = (jnp.minimum(logits, 0.0) - jnp.log1p(jnp.exp(-jnp.abs(logits)))) / DECAY_POWER

    def level(b):
        row = lax.broadcasted_iota(jnp.int32, (rows, 1), 0)
        pos = (row + (chip * 2 + b) * rows + (1 - seq // 2)).astype(F32)
        return pos * log_decay

    def scan_copy(phase, p, d, src, dst, axis, at, n):
        to = lax.rem(at + d, n)
        return remote(src, dst, scan_s.at[phase, p, d - 1], scan_r.at[phase, p, d - 1], {axis: to})

    def a_send(p, d):
        return scan_copy(0, p, d, sa.at[p, lax.rem(x + d, nx)], ra.at[p, x], X, x, nx)

    def a_recv(p, d):
        at = lax.rem(x + nx - d, nx)
        return scan_copy(0, p, d, sa.at[p, at], ra.at[p, at], X, x, nx)

    def b_send(p, d):
        return scan_copy(1, p, d, tb.at[p], rb.at[p, y], Y, y, ny)

    def b_recv(p, d):
        return scan_copy(1, p, d, tb.at[p], rb.at[p, lax.rem(y + ny - d, ny)], Y, y, ny)

    def c_send(p, d):
        return scan_copy(2, p, d, tc.at[p], rc.at[p, z], Z, z, nz)

    def c_recv(p, d):
        return scan_copy(2, p, d, tc.at[p], rc.at[p, lax.rem(z + nz - d, nz)], Z, z, nz)

    def d_send(p, d):
        return scan_copy(3, p, d, dd.at[p, lax.rem(x + d, nx)], pd.at[p, x], X, x, nx)

    def d_recv(p, d):
        at = lax.rem(x + nx - d, nx)
        return scan_copy(3, p, d, dd.at[p, at], pd.at[p, at], X, x, nx)

    def scan_a(p):
        for h in range(2):
            state = (sb[0, 2 * p + h] + sb[1, 2 * p + h]).astype(BF16)
            for i in range(nx):
                sa[p, i, h] = state[i * chunk : (i + 1) * chunk]
        for d in range(1, nx):
            a_send(p, d).start()
        ra[p, x] = sa[p, x]

    def scan_b(p):
        for d in range(1, nx):
            a_recv(p, d).wait_recv()
        total = ra[p, 0].astype(F32)
        for i in range(1, nx):
            total += ra[p, i].astype(F32)
        tb[p] = total.astype(BF16)
        for d in range(1, ny):
            b_send(p, d).start()
        rb[p, y] = tb[p]

    def scan_c(p):
        for d in range(1, ny):
            b_recv(p, d).wait_recv()
        total = jnp.zeros(tb.shape[1:], F32)
        before = jnp.zeros(tb.shape[1:], F32)
        for i in range(ny):
            part = rb[p, i].astype(F32)
            total += part
            before += jnp.where(i < y, part, 0.0)
        yp[p] = before
        tc[p] = total.astype(BF16)
        for d in range(1, nz):
            c_send(p, d).start()
        rc[p, z] = tc[p]

    def scan_d(p):
        for d in range(1, nz):
            c_recv(p, d).wait_recv()
        before = yp[p]
        for i in range(nz):
            before += jnp.where(i < z, rc[p, i].astype(F32), 0.0)
        for i in range(nx):
            dd[p, i] = before.astype(BF16)
            before += ra[p, i].astype(F32)
        for d in range(1, nx):
            d_send(p, d).start()
        pd[p, x] = dd[p, x]

    def scan_end(p):
        for d in range(1, nx):
            d_recv(p, d).wait_recv()

    @pl.loop(0, 2)
    def _(j):
        b = lax.rem(c + j, 2)

        @pl.when(j == 0)
        def _():
            wk_copy.wait()

        @pl.when(j == 1)
        def _():
            for i in range(token_steps):
                x_recv(i).wait_recv()

        keys = dot(xn[b], wkb[...]) * jnp.exp(-level(b))
        for h in range(heads):
            kb[b, h] = keys[:, h * HEAD_K : (h + 1) * HEAD_K].astype(BF16)
        for n in range(vsteps):

            @pl.when(j == 0)
            def _():
                wv_copy[n].wait()

            values = dot(xn[b], wvb[n]).astype(BF16)
            for i in range(2):
                h = 2 * n + i
                v = values[:, i * HEAD_V : (i + 1) * HEAD_V]
                vb[b, h] = v
                sb[b, h] = dot(kb[b, h], v, ((0,), (0,)))

            @pl.when(j == 1)
            def _():
                scan_a(n)

    wq_copy.wait()

    @pl.loop(0, 2)
    def _(b):
        queries = dot(xn[b], wqb[...]) * (jnp.exp(level(b)) * HEAD_K**-0.5)
        for h in range(heads):
            qb[b, h] = queries[:, h * HEAD_K : (h + 1) * HEAD_K].astype(BF16)

    def wo_send(n):
        return remote(wob.at[n], wpb.at[n], ps.at[n], pr.at[n], {TP: other})

    for n in range(osteps):
        wo_copy[n].wait()
        wo_send(n).start()

    for n in range(vsteps):
        wg_copy[n].wait()
    scan_b(0)

    @pl.loop(0, 2)
    def _(b):
        for n in range(vsteps):
            u = dot(xn[b], wgb[n])
            u = u / (1.0 + jnp.exp(-u)) * hgainb[:, n * UNIT : (n + 1) * UNIT]
            for i in range(2):
                gsb[b, 2 * n + i] = u[:, i * HEAD_V : (i + 1) * HEAD_V]

            if n == 0:

                @pl.when(b == 0)
                def _():
                    scan_b(1)

                @pl.when(b == 1)
                def _():
                    scan_c(0)

    scan_c(1)

    @pl.loop(0, heads)
    def _(h):
        for b in range(2):
            scores = dot(qb[b, h], kb[b, h], ((1,), (1,)))
            i = lax.broadcasted_iota(jnp.int32, scores.shape, 0)
            j = lax.broadcasted_iota(jnp.int32, scores.shape, 1)
            scores = jnp.where(i >= j, scores, 0.0).astype(BF16)
            lob[b, h] = dot(scores, vb[b, h])

    scan_d(0)
    scan_d(1)

    def g_send(h):
        p, i = divmod(h, 2)
        return remote(
            gsnd.at[p, i], grcv.at[p, i], gs_s.at[h], gs_r.at[h], {TP: other}
        )

    for p in range(pairs):
        scan_end(p)
        for i in range(2):
            h = 2 * p + i
            carried = pd[p, :, i].astype(F32).reshape(HEAD_K, HEAD_V)
            for own in range(2):
                b = c if own else other
                state = carried + jnp.where(b == 1, sb[0, h], 0.0)
                o = lob[b, h] + dot(qb[b, h], state.astype(BF16))
                scale = lax.rsqrt(jnp.mean(o * o, axis=-1, keepdims=True) + EPS)
                gated = (o * scale * gsb[b, h]).astype(BF16)
                if own:
                    gown[p, i] = gated
                else:
                    gsnd[p, i] = gated
                    g_send(h).start()
        if p == 0:
            for n in range(osteps):
                wo_send(n).wait_recv()
        for i in range(2):
            g_send(2 * p + i).wait_recv()

        @pl.loop(0, osteps)
        def _(n):
            part = acc[n] if p else None
            for i in range(2):
                r = slice((2 * p + i) * HEAD_V, (2 * p + i + 1) * HEAD_V)
                term = dot(gown[p, i], wob[n, r, :]) + dot(grcv[p, i], wpb[n, r, :])
                part = term if part is None else part + term
            if p < pairs - 1:
                acc[n] = part
            else:
                ost[n] = part.astype(BF16)

    for n in range(osteps):
        pltpu.make_async_copy(ost.at[n], out.at[:, cols(n)], out_sem.at[n]).start()
    for n in range(osteps):
        pltpu.make_async_copy(ost.at[n], out.at[:, cols(n)], out_sem.at[n]).wait()

    for i in range(token_steps):
        x_send(i).wait_send()
    for n in range(osteps):
        wo_send(n).wait_send()
    for h in range(heads):
        g_send(h).wait_send()
    for p in range(pairs):
        for d in range(1, nx):
            a_send(p, d).wait_send()
            d_send(p, d).wait_send()
        for d in range(1, ny):
            b_send(p, d).wait_send()
        for d in range(1, nz):
            c_send(p, d).wait_send()


def on_device(sizes, tok, gain, wq, wk, wv, wg, bias, hgain, wo):
    nz, ny, nx = sizes
    rows, width = tok.shape
    key_width, value_width, model = wq.shape[1], wv.shape[1], wo.shape[1]
    heads = key_width // HEAD_K
    pairs = heads // 2
    chunk = HEAD_K // nx
    vsteps, osteps = value_width // UNIT, model // UNIT
    token_steps = 4
    most = max(sizes) - 1
    vmem = pltpu.VMEM
    dma = pltpu.SemaphoreType.DMA
    quarter = (2, chunk, HEAD_V)
    scratch = [
        vmem((2, rows, width), BF16),
        vmem((width, key_width), BF16),
        vmem((vsteps, width, UNIT), BF16),
        vmem((width, key_width), BF16),
        vmem((vsteps, width, UNIT), BF16),
        vmem((osteps, value_width, UNIT), BF16),
        vmem((osteps, value_width, UNIT), BF16),
        vmem((1, width), F32),
        vmem((1, key_width), F32),
        vmem((1, value_width), F32),
        vmem((2, heads, rows, HEAD_K), BF16),
        vmem((2, heads, rows, HEAD_K), BF16),
        vmem((2, heads, rows, HEAD_V), BF16),
        vmem((2, heads, rows, HEAD_V), F32),
        vmem((2, heads, rows, HEAD_V), F32),
        vmem((2, heads, HEAD_K, HEAD_V), F32),
        vmem((osteps, rows, UNIT), F32),
        vmem((osteps, rows, UNIT), BF16),
        vmem((pairs, nx, *quarter), BF16),
        vmem((pairs, nx, *quarter), BF16),
        vmem((pairs, *quarter), BF16),
        vmem((pairs, ny, *quarter), BF16),
        vmem((pairs, *quarter), F32),
        vmem((pairs, *quarter), BF16),
        vmem((pairs, nz, *quarter), BF16),
        vmem((pairs, nx, *quarter), BF16),
        vmem((pairs, nx, *quarter), BF16),
        vmem((pairs, 2, rows, HEAD_V), BF16),
        vmem((pairs, 2, rows, HEAD_V), BF16),
        vmem((pairs, 2, rows, HEAD_V), BF16),
        dma((token_steps,)),
        dma((2 + 2 * vsteps,)),
        dma((3,)),
        dma((osteps,)),
        dma((osteps,)),
        dma((token_steps,)),
        dma((token_steps,)),
        dma((osteps,)),
        dma((osteps,)),
        dma((heads,)),
        dma((heads,)),
        dma((4, pairs, most)),
        dma((4, pairs, most)),
    ]
    hbm = pl.BlockSpec(memory_space=pl.ANY)
    return pl.pallas_call(
        functools.partial(mixer, sizes),
        out_shape=jax.ShapeDtypeStruct((rows, model), BF16),
        in_specs=[hbm] * 9,
        out_specs=hbm,
        scratch_shapes=scratch,
        compiler_params=pltpu.CompilerParams(
            collective_id=0, has_side_effects=True, vmem_limit_bytes=67_043_328
        ),
        name="mixer",
    )(
        tok, gain.reshape(1, -1), wq, wk, wv, wg, bias.reshape(1, -1), hgain.reshape(1, -1), wo
    )


def solution(mesh, sizes=(4, 4, 4)):
    finer = Mesh(mesh.devices.reshape(*sizes, mesh.shape["tp"]), SP_TP)
    in_specs = (
        P(SP_TP, None),
        P(),
        P(None, "tp"),
        P(None, "tp"),
        P(None, "tp"),
        P(None, "tp"),
        P("tp"),
        P("tp"),
        P("tp", None),
    )
    return jax.shard_map(
        functools.partial(on_device, sizes),
        mesh=finer,
        in_specs=in_specs,
        out_specs=P(SP_TP, None),
        check_vma=False,
    )
```

```python
import functools
import math

import jax
import jax.numpy as jnp
from jax import lax
from jax.experimental import pallas as pl
from jax.experimental.pallas import tpu as pltpu
from jax.sharding import Mesh
from jax.sharding import PartitionSpec as P

HEAD_K = 128
HEAD_V = 256
Z, Y, X, TP = "sp_0", "sp_1", "sp_2", "tp"
SP_TP = (Z, Y, X, TP)
MESH = pl.DeviceIdType.MESH
UNIT = 512
EPS = 1e-06
DECAY_POWER = 16.0
F32, BF16 = jnp.float32, jnp.bfloat16


def remote(src, dst, send, recv, where):
    return pltpu.make_async_remote_copy(
        src_ref=src, dst_ref=dst, send_sem=send, recv_sem=recv, device_id=where, device_id_type=MESH
    )


def dot(a, b, dims=((1,), (0,))):
    return lax.dot_general(a, b, (dims, ((), ())), preferred_element_type=F32)


def mixer(
    sizes,
    tok, gain, wq, wk, wv, wg, bias, hgain, wo,
    out,
    xn, wkb, wvb, wqb, wgb, wob, gainb, biasb, hgainb,
    kb, qb, vb, gsb, lob, acc,
    sa, ra, tb, rb, yp, tc, rc, dd, pd,
    gall, gsnd,
    tok_sem, small_sem, k_sem, v_sem, q_sem, g_sem, wo_sem,
    xs, xr, ps, pr, gs_s, gs_r, scan_s, scan_r,
):
    nz, ny, nx = sizes
    rows, width = xn.shape[1], xn.shape[2]
    heads = kb.shape[1]
    pairs = heads // 2
    chunk = HEAD_K // nx
    token_steps = tok_sem.shape[0]
    step_rows = rows // token_steps
    model = out.shape[1]
    z, y, x, c = (lax.axis_index(a) for a in SP_TP)
    other = 1 - c
    chip = (z * ny + y) * nx + x
    seq = nz * ny * nx * 2 * rows

    def token_copy(i):
        r = pl.ds(i * step_rows, step_rows)
        return pltpu.make_async_copy(tok.at[r, :], xn.at[c, r, :], tok_sem.at[i])

    small = [(gain, gainb), (bias, biasb), (hgain, hgainb)]
    small = [pltpu.make_async_copy(a, b, small_sem.at[i]) for i, (a, b) in enumerate(small)]
    v2 = 2 * HEAD_V
    wk_copy = pltpu.make_async_copy(wk, wkb, k_sem.at[0])
    wv_copy = [pltpu.make_async_copy(wv.at[:, pl.ds(p * v2, v2)], wvb.at[p], v_sem.at[p]) for p in range(pairs)]
    wq_copy = pltpu.make_async_copy(wq, wqb, q_sem.at[0])
    wg_copy = [pltpu.make_async_copy(wg.at[:, pl.ds(p * v2, v2)], wgb.at[p], g_sem.at[p]) for p in range(pairs)]

    def wo_copy(h):
        return pltpu.make_async_copy(wo.at[pl.ds(h * HEAD_V, HEAD_V), :], wob.at[h, 0], wo_sem.at[h])

    def wo_send(h):
        return remote(wob.at[h, 0], wob.at[h, 1], ps.at[h], pr.at[h], {TP: other})

    for s in small:
        s.start()
    for i in range(token_steps):
        token_copy(i).start()
    wk_copy.start(priority=1)

    barrier = pltpu.get_barrier_semaphore()
    peers = [{TP: other}]
    peers += [{X: lax.rem(x + d, nx)} for d in range(1, nx)]
    peers += [{Y: lax.rem(y + d, ny)} for d in range(1, ny)]
    peers += [{Z: lax.rem(z + d, nz)} for d in range(1, nz)]
    for peer in peers:
        pl.semaphore_signal(barrier, inc=1, device_id=peer, device_id_type=MESH)

    def x_send(i):
        r = pl.ds(i * step_rows, step_rows)
        return remote(xn.at[c, r, :], xn.at[c, r, :], xs.at[i], xr.at[i], {TP: other})

    def x_recv(i):
        r = pl.ds(i * step_rows, step_rows)
        return remote(xn.at[other, r, :], xn.at[other, r, :], xs.at[i], xr.at[i], {TP: other})

    for s in small:
        s.wait()
    for i in range(token_steps):
        token_copy(i).wait()
        if i == token_steps - 1:
            for s in wv_copy:
                s.start(priority=1)

        for g in range(step_rows // 16):
            r = pl.ds(i * step_rows + g * 16, 16)
            v = xn[c, r, :].astype(F32)
            scale = lax.rsqrt(jnp.mean(v * v, axis=-1, keepdims=True) + EPS)
            v = xn[c, r, :].astype(F32)
            xn[c, r, :] = (v * scale * gainb[...]).astype(BF16)

        if i == 0:
            pl.semaphore_wait(barrier, len(peers))
        x_send(i).start()

    logits = biasb[...] + math.log(seq / 8.0)
    log_decay = (jnp.minimum(logits, 0.0) - jnp.log1p(jnp.exp(-jnp.abs(logits)))) / DECAY_POWER

    def level(b):
        row = lax.broadcasted_iota(jnp.int32, (rows, 1), 0)
        pos = (row + (chip * 2 + b) * rows + (1 - seq // 2)).astype(F32)
        return pos * log_decay

    def scan_copy(phase, h, d, src, dst, axis, at, n):
        to = lax.rem(at + d, n)
        return remote(src, dst, scan_s.at[phase, h, d - 1], scan_r.at[phase, h, d - 1], {axis: to})

    def a_send(h, d):
        return scan_copy(0, h, d, sa.at[h, lax.rem(x + d, nx)], ra.at[h, x], X, x, nx)

    def a_recv(h, d):
        at = lax.rem(x + nx - d, nx)
        return scan_copy(0, h, d, sa.at[h, at], ra.at[h, at], X, x, nx)

    def b_send(h, d):
        return scan_copy(1, h, d, tb.at[h], rb.at[h, y], Y, y, ny)

    def b_recv(h, d):
        return scan_copy(1, h, d, tb.at[h], rb.at[h, lax.rem(y + ny - d, ny)], Y, y, ny)

    def c_send(h, d):
        return scan_copy(2, h, d, tc.at[h], rc.at[h, d - 1], Z, z, nz)

    def c_recv(h, d):
        return scan_copy(2, h, d, tc.at[h], rc.at[h, d - 1], Z, z, nz)

    def d_send(h, d):
        return scan_copy(3, h, d, dd.at[h, lax.rem(x + d, nx)], pd.at[h, x], X, x, nx)

    def d_recv(h, d):
        at = lax.rem(x + nx - d, nx)
        return scan_copy(3, h, d, dd.at[h, at], pd.at[h, at], X, x, nx)

    far_first = lambda n: [2, 1, 3] if n == 4 else list(range(1, n))

    def scan_a(h):
        k = kb[:, h].reshape(2 * rows, HEAD_K)
        v = vb[:, h].reshape(2 * rows, HEAD_V)
        sa[h] = dot(k, v, ((0,), (0,))).astype(BF16).reshape(nx, chunk, HEAD_V)
        for d in far_first(nx):
            a_send(h, d).start()
        ra[h, x] = sa[h, x]

    def scan_b(h):
        for d in range(1, nx):
            a_recv(h, d).wait_recv()
        total = ra[h, 0].astype(F32)
        for i in range(1, nx):
            total += ra[h, i].astype(F32)
        tb[h] = total.astype(BF16)
        for d in far_first(ny):
            b_send(h, d).start()
        rb[h, y] = tb[h]

    def scan_c(h):
        for d in range(1, ny):
            b_recv(h, d).wait_recv()
        total = jnp.zeros(tb.shape[1:], F32)
        before = jnp.zeros(tb.shape[1:], F32)
        for i in range(ny):
            part = rb[h, i].astype(F32)
            total += part
            before += jnp.where(i < y, part, 0.0)
        tc[h] = total.astype(BF16)
        for d in far_first(nz):

            @pl.when(z + d < nz)
            def _():
                c_send(h, d).start()

        yp[h] = before

    def scan_d(h):
        for d in range(1, nz):

            @pl.when(z >= d)
            def _():
                c_recv(h, d).wait_recv()
                yp[h] += rc[h, d - 1].astype(F32)

        before = yp[h]
        for i in range(nx):
            dd[h, i] = before.astype(BF16)
            before += ra[h, i].astype(F32)
        for d in far_first(nx):
            d_send(h, d).start()
        pd[h, x] = dd[h, x]

    def scan_end(h):
        for d in range(1, nx):
            d_recv(h, d).wait_recv()

    def keys(b):
        k = dot(xn[b], wkb[...]) * jnp.exp(-level(b))
        for h in range(heads):
            kb[b, h] = k[:, h * HEAD_K : (h + 1) * HEAD_K].astype(BF16)

    def values(b, p):
        v = dot(xn[b], wvb[p]).astype(BF16)
        for i in range(2):
            vb[b, 2 * p + i] = v[:, i * HEAD_V : (i + 1) * HEAD_V]

    wk_copy.wait()
    keys(c)
    for h in range(heads):
        wo_copy(h).start(priority=1)
    wv_copy[0].wait()
    values(c, 0)
    wv_copy[1].wait()
    wq_copy.start(priority=1)
    for s in wg_copy:
        s.start(priority=1)
    values(c, 1)
    for i in range(token_steps):
        x_recv(i).wait_recv()
    keys(other)
    values(other, 0)
    scan_a(0)
    scan_a(1)
    wo_copy(0).wait()
    wo_send(0).start()
    values(other, 1)
    scan_a(2)
    scan_a(3)

    def queries(b):
        q = dot(xn[b], wqb[...]) * (jnp.exp(level(b)) * HEAD_K**-0.5)
        for h in range(heads):
            qb[b, h] = q[:, h * HEAD_K : (h + 1) * HEAD_K].astype(BF16)

    def gates(b, p):
        u = dot(xn[b], wgb[p])
        u = u / (1.0 + jnp.exp(-u)) * hgainb[:, p * v2 : (p + 1) * v2]
        for i in range(2):
            gsb[b, 2 * p + i] = u[:, i * HEAD_V : (i + 1) * HEAD_V].astype(BF16)

    def local(h):
        i = lax.broadcasted_iota(jnp.int32, (rows, rows), 0)
        j = lax.broadcasted_iota(jnp.int32, (rows, rows), 1)
        for b in range(2):
            scores = dot(qb[b, h], kb[b, h], ((1,), (1,)))
            scores = jnp.where(i >= j, scores, 0.0).astype(BF16)
            o = dot(scores, vb[b, h])
            if b:
                scores = dot(qb[b, h], kb[0, h], ((1,), (1,))).astype(BF16)
                o += dot(scores, vb[0, h])
            lob[b, h] = o.astype(BF16)

    wq_copy.wait()
    queries(0)
    scan_b(0)
    wo_copy(1).wait()
    wo_send(1).start()
    queries(1)
    scan_b(1)
    for s in wg_copy:
        s.wait()
    gates(0, 0)
    scan_b(2)
    scan_b(3)
    scan_c(0)
    wo_copy(2).wait()
    wo_send(2).start()
    gates(1, 0)
    scan_c(1)
    gates(0, 1)
    scan_c(2)
    scan_c(3)
    local(0)
    local(1)
    scan_d(0)
    wo_copy(3).wait()
    wo_send(3).start()
    gates(1, 1)
    scan_d(1)
    local(2)
    local(3)
    scan_d(2)
    scan_d(3)

    def g_send(h):
        return remote(gsnd.at[h], gall.at[h, 1], gs_s.at[h], gs_r.at[h], {TP: other})

    def carried(h):
        start = pd[h].reshape(HEAD_K, HEAD_V)
        for own in (False, True):
            b = c if own else other
            o = lob[b, h].astype(F32) + dot(qb[b, h], start)
            scale = lax.rsqrt(jnp.mean(o * o, axis=-1, keepdims=True) + EPS)
            gated = (o * scale * gsb[b, h].astype(F32)).astype(BF16)
            if own:
                gall[h, 0] = gated
            else:
                gsnd[h] = gated
                g_send(h).start()

    def project(h):
        gated = jnp.concatenate([gall[h, 0], gall[h, 1]], axis=1)
        for n in range(model // UNIT):
            at = slice(n * UNIT, (n + 1) * UNIT)
            part = dot(gated, wob[h, :, :, at].reshape(2 * HEAD_V, UNIT))
            if h:
                part += acc[n]
            if h < heads - 1:
                acc[n] = part
            else:
                out[:, at] = part.astype(BF16)

    scan_end(0)
    carried(0)
    for h in range(1, heads + 1):
        if h < heads:
            scan_end(h)
        g_send(h - 1).wait_recv()
        wo_send(h - 1).wait_recv()
        if h < heads:
            carried(h)
        project(h - 1)

    for i in range(token_steps):
        x_send(i).wait_send()
    for h in range(heads):
        wo_send(h).wait_send()
        g_send(h).wait_send()
        for d in range(1, nx):
            a_send(h, d).wait_send()
            d_send(h, d).wait_send()
        for d in range(1, ny):
            b_send(h, d).wait_send()
        for d in range(1, nz):

            @pl.when(z + d < nz)
            def _():
                c_send(h, d).wait_send()


def on_device(sizes, tok, gain, wq, wk, wv, wg, bias, hgain, wo):
    nz, ny, nx = sizes
    rows, width = tok.shape
    key_width, value_width, model = wq.shape[1], wv.shape[1], wo.shape[1]
    heads = key_width // HEAD_K
    pairs = heads // 2
    token_steps = 4
    most = max(sizes) - 1
    vmem = pltpu.VMEM
    dma = pltpu.SemaphoreType.DMA
    quarter = (HEAD_K // nx, HEAD_V)
    scratch = [
        vmem((2, rows, width), BF16),
        vmem((width, key_width), BF16),
        vmem((pairs, width, 2 * HEAD_V), BF16),
        vmem((width, key_width), BF16),
        vmem((pairs, width, 2 * HEAD_V), BF16),
        vmem((heads, 2, HEAD_V, model), BF16),
        vmem((1, width), F32),
        vmem((1, key_width), F32),
        vmem((1, value_width), F32),
        vmem((2, heads, rows, HEAD_K), BF16),
        vmem((2, heads, rows, HEAD_K), BF16),
        vmem((2, heads, rows, HEAD_V), BF16),
        vmem((2, heads, rows, HEAD_V), BF16),
        vmem((2, heads, rows, HEAD_V), BF16),
        vmem((model // UNIT, rows, UNIT), F32),
        vmem((heads, nx, *quarter), BF16),
        vmem((heads, nx, *quarter), BF16),
        vmem((heads, *quarter), BF16),
        vmem((heads, ny, *quarter), BF16),
        vmem((heads, *quarter), F32),
        vmem((heads, *quarter), BF16),
        vmem((heads, nz - 1, *quarter), BF16),
        vmem((heads, nx, *quarter), BF16),
        vmem((heads, nx, *quarter), BF16),
        vmem((heads, 2, rows, HEAD_V), BF16),
        vmem((heads, rows, HEAD_V), BF16),
        dma((token_steps,)),
        dma((3,)),
        dma((1,)),
        dma((pairs,)),
        dma((1,)),
        dma((pairs,)),
        dma((heads,)),
        dma((token_steps,)),
        dma((token_steps,)),
        dma((heads,)),
        dma((heads,)),
        dma((heads,)),
        dma((heads,)),
        dma((4, heads, most)),
        dma((4, heads, most)),
    ]
    hbm = pl.BlockSpec(memory_space=pl.ANY)
    return pl.pallas_call(
        functools.partial(mixer, sizes),
        out_shape=pltpu.VMEM((rows, model), BF16),
        in_specs=[hbm] * 9,
        out_specs=pl.BlockSpec(memory_space=pltpu.VMEM),
        scratch_shapes=scratch,
        compiler_params=pltpu.CompilerParams(
            collective_id=0, has_side_effects=True, vmem_limit_bytes=64_500_000
        ),
        name="mixer",
    )(
        tok, gain.reshape(1, -1), wq, wk, wv, wg, bias.reshape(1, -1), hgain.reshape(1, -1), wo
    )


def solution(mesh, sizes=(4, 4, 4)):
    finer = Mesh(mesh.devices.reshape(*sizes, mesh.shape["tp"]), SP_TP)
    in_specs = (
        P(SP_TP, None),
        P(),
        P(None, "tp"),
        P(None, "tp"),
        P(None, "tp"),
        P(None, "tp"),
        P("tp"),
        P("tp"),
        P("tp", None),
    )
    return jax.shard_map(
        functools.partial(on_device, sizes),
        mesh=finer,
        in_specs=in_specs,
        out_specs=P(SP_TP, None),
        check_vma=False,
    )
```

```python
import functools
import math

import jax
import jax.numpy as jnp
from jax import lax
from jax.experimental import pallas as pl
from jax.experimental.pallas import tpu as pltpu
from jax.sharding import Mesh
from jax.sharding import PartitionSpec as P

HEAD_K = 128
HEAD_V = 256
Z, Y, X, TP = "sp_0", "sp_1", "sp_2", "tp"
SP_TP = (Z, Y, X, TP)
MESH = pl.DeviceIdType.MESH
UNIT = 512
EPS = 1e-06
DECAY_POWER = 16.0
F32, BF16 = jnp.float32, jnp.bfloat16


def remote(src, dst, send, recv, where):
    return pltpu.make_async_remote_copy(
        src_ref=src, dst_ref=dst, send_sem=send, recv_sem=recv, device_id=where, device_id_type=MESH
    )


def dot(a, b, dims=((1,), (0,))):
    return lax.dot_general(a, b, (dims, ((), ())), preferred_element_type=F32)


def mixer(
    sizes,
    tok, gain, wq, wk, wv, wg, bias, hgain, wo,
    out,
    xn, wkb, wvb, wqb, wgb, wob, gainb, biasb, hgainb,
    kb, qb, vb, gsb, lob, acc,
    sa, ra, tb, rb, yp, tc, rc, dd, pd,
    gall, gsnd,
    tok_sem, small_sem, k_sem, v_sem, q_sem, g_sem, wo_sem,
    xs, xr, ps, pr, gs_s, gs_r, scan_s, scan_r, zsem,
):
    nz, ny, nx = sizes
    rows, width = xn.shape[1], xn.shape[2]
    heads = kb.shape[1]
    pairs = heads // 2
    chunk = HEAD_K // nx
    token_steps = tok_sem.shape[0]
    step_rows = rows // token_steps
    model = out.shape[1]
    z, y, x, c = (lax.axis_index(a) for a in SP_TP)
    other = 1 - c
    chip = (z * ny + y) * nx + x
    seq = nz * ny * nx * 2 * rows

    def token_copy(i):
        r = pl.ds(i * step_rows, step_rows)
        return pltpu.make_async_copy(tok.at[r, :], xn.at[c, r, :], tok_sem.at[i])

    small = [(gain, gainb), (bias, biasb), (hgain, hgainb)]
    small = [pltpu.make_async_copy(a, b, small_sem.at[i]) for i, (a, b) in enumerate(small)]
    v2 = 2 * HEAD_V
    wk_copy = pltpu.make_async_copy(wk, wkb, k_sem.at[0])
    wv_copy = [pltpu.make_async_copy(wv.at[:, pl.ds(p * v2, v2)], wvb.at[p], v_sem.at[p]) for p in range(pairs)]
    wq_copy = pltpu.make_async_copy(wq, wqb, q_sem.at[0])
    wg_copy = [pltpu.make_async_copy(wg.at[:, pl.ds(p * v2, v2)], wgb.at[p], g_sem.at[p]) for p in range(pairs)]

    def wo_copy(h):
        return pltpu.make_async_copy(wo.at[pl.ds(h * HEAD_V, HEAD_V), :], wob.at[h, 0], wo_sem.at[h])

    def wo_send(h):
        return remote(wob.at[h, 0], wob.at[h, 1], ps.at[h], pr.at[h], {TP: other})

    for s in small:
        s.start()
    for i in range(token_steps):
        token_copy(i).start()
    wk_copy.start(priority=1)

    barrier = pltpu.get_barrier_semaphore()
    peers = [{TP: other}]
    peers += [{X: lax.rem(x + d, nx)} for d in range(1, nx)]
    peers += [{Y: lax.rem(y + d, ny)} for d in range(1, ny)]
    for peer in peers:
        pl.semaphore_signal(barrier, inc=1, device_id=peer, device_id_type=MESH)
    for d in range(1, nz):

        @pl.when(z + d < nz)
        def _():
            pl.semaphore_signal(barrier, inc=1, device_id={Z: lax.rem(z + d, nz)}, device_id_type=MESH)

    def x_send(i):
        r = pl.ds(i * step_rows, step_rows)
        return remote(xn.at[c, r, :], xn.at[c, r, :], xs.at[i], xr.at[i], {TP: other})

    def x_recv(i):
        r = pl.ds(i * step_rows, step_rows)
        return remote(xn.at[other, r, :], xn.at[other, r, :], xs.at[i], xr.at[i], {TP: other})

    for s in small:
        s.wait()
    for i in range(token_steps):
        token_copy(i).wait()
        if i == token_steps - 1:
            for s in wv_copy:
                s.start(priority=1)

        for g in range(step_rows // 16):
            r = pl.ds(i * step_rows + g * 16, 16)
            v = xn[c, r, :].astype(F32)
            scale = lax.rsqrt(jnp.mean(v * v, axis=-1, keepdims=True) + EPS)
            v = xn[c, r, :].astype(F32)
            xn[c, r, :] = (v * scale * gainb[...]).astype(BF16)


    pl.semaphore_wait(barrier, len(peers) + z)
    for i in range(token_steps):
        x_send(i).start()
    for d in range(1, nz):

        @pl.when(z >= d)
        def _():
            pl.semaphore_signal(zsem, inc=1, device_id={Z: lax.rem(z - d + nz, nz)}, device_id_type=MESH)


    logits = biasb[...] + math.log(seq / 8.0)
    log_decay = (jnp.minimum(logits, 0.0) - jnp.log1p(jnp.exp(-jnp.abs(logits)))) / DECAY_POWER

    def level(b):
        row = lax.broadcasted_iota(jnp.int32, (rows, 1), 0)
        pos = (row + (chip * 2 + b) * rows + (1 - seq // 2)).astype(F32)
        return pos * log_decay

    def scan_copy(phase, h, d, src, dst, axis, at, n):
        to = lax.rem(at + d, n)
        return remote(src, dst, scan_s.at[phase, h, d - 1], scan_r.at[phase, h, d - 1], {axis: to})

    def a_send(h, d):
        return scan_copy(0, h, d, sa.at[h, lax.rem(x + d, nx)], ra.at[h, x], X, x, nx)

    def a_recv(h, d):
        at = lax.rem(x + nx - d, nx)
        return scan_copy(0, h, d, sa.at[h, at], ra.at[h, at], X, x, nx)

    def b_send(h, d):
        return scan_copy(1, h, d, tb.at[h], rb.at[h, y], Y, y, ny)

    def b_recv(h, d):
        return scan_copy(1, h, d, tb.at[h], rb.at[h, lax.rem(y + ny - d, ny)], Y, y, ny)

    def c_send(h, d):
        return scan_copy(2, h, d, tc.at[h], rc.at[h, d - 1], Z, z, nz)

    def c_recv(h, d):
        return scan_copy(2, h, d, tc.at[h], rc.at[h, d - 1], Z, z, nz)

    def d_send(h, d):
        return scan_copy(3, h, d, dd.at[h, lax.rem(x + d, nx)], pd.at[h, x], X, x, nx)

    def d_recv(h, d):
        at = lax.rem(x + nx - d, nx)
        return scan_copy(3, h, d, dd.at[h, at], pd.at[h, at], X, x, nx)

    far_first = lambda n: [2, 1, 3] if n == 4 else list(range(1, n))

    def scan_a(pair):
        for h in pair:
            k = kb[:, h].reshape(2 * rows, HEAD_K)
            v = vb[:, h].reshape(2 * rows, HEAD_V)
            sa[h] = dot(k, v, ((0,), (0,))).astype(BF16).reshape(nx, chunk, HEAD_V)
        for h in pair:
            for d in far_first(nx):
                a_send(h, d).start()
        for h in pair:
            ra[h, x] = sa[h, x]

    def scan_b(h):
        for d in range(1, nx):
            a_recv(h, d).wait_recv()
        total = ra[h, 0].astype(F32)
        for i in range(1, nx):
            total += ra[h, i].astype(F32)
        tb[h] = total.astype(BF16)
        for d in far_first(ny):
            b_send(h, d).start()
        rb[h, y] = tb[h]

    def scan_c(h):
        for d in range(1, ny):
            b_recv(h, d).wait_recv()
        total = jnp.zeros(tb.shape[1:], F32)
        before = jnp.zeros(tb.shape[1:], F32)
        for i in range(ny):
            part = rb[h, i].astype(F32)
            total += part
            before += jnp.where(i < y, part, 0.0)
        tc[h] = total.astype(BF16)
        for d in far_first(nz):

            @pl.when(z + d < nz)
            def _():
                c_send(h, d).start()

        yp[h] = before

        @pl.when(z == 0)
        def _():
            scan_back(h)

    def scan_d(h):
        @pl.when(z > 0)
        def _():
            scan_z(h)
            scan_back(h)

    def scan_z(h):
        for d in range(1, nz):

            @pl.when(z >= d)
            def _():
                c_recv(h, d).wait_recv()
                yp[h] += rc[h, d - 1].astype(F32)

    def scan_back(h):
        before = yp[h]
        for i in range(nx):
            dd[h, i] = before.astype(BF16)
            before += ra[h, i].astype(F32)
        for d in far_first(nx):
            d_send(h, d).start()
        pd[h, x] = dd[h, x]

    def scan_end(h):
        for d in range(1, nx):
            d_recv(h, d).wait_recv()

    def keys(b):
        k = dot(xn[b], wkb[...]) * jnp.exp(-level(b))
        for h in range(heads):
            kb[b, h] = k[:, h * HEAD_K : (h + 1) * HEAD_K].astype(BF16)

    def values(b, p):
        v = dot(xn[b], wvb[p]).astype(BF16)
        for i in range(2):
            vb[b, 2 * p + i] = v[:, i * HEAD_V : (i + 1) * HEAD_V]

    wk_copy.wait()
    keys(c)
    for h in range(heads):
        wo_copy(h).start(priority=1)
    wv_copy[0].wait()
    values(c, 0)
    wv_copy[1].wait()
    wq_copy.start(priority=1)
    for s in wg_copy:
        s.start(priority=1)
    values(c, 1)
    for i in range(token_steps):
        x_recv(i).wait_recv()
    keys(other)
    values(other, 0)
    scan_a((0, 1))
    wo_copy(0).wait()
    wo_send(0).start()
    values(other, 1)
    scan_a((2, 3))

    def queries(b):
        q = dot(xn[b], wqb[...]) * (jnp.exp(level(b)) * HEAD_K**-0.5)
        for h in range(heads):
            qb[b, h] = q[:, h * HEAD_K : (h + 1) * HEAD_K].astype(BF16)

    def gates(b, p):
        u = dot(xn[b], wgb[p])
        u = u / (1.0 + jnp.exp(-u)) * hgainb[:, p * v2 : (p + 1) * v2]
        for i in range(2):
            gsb[b, 2 * p + i] = u[:, i * HEAD_V : (i + 1) * HEAD_V].astype(BF16)

    def local(h):
        i = lax.broadcasted_iota(jnp.int32, (rows, rows), 0)
        j = lax.broadcasted_iota(jnp.int32, (rows, rows), 1)
        for b in range(2):
            scores = dot(qb[b, h], kb[b, h], ((1,), (1,)))
            scores = jnp.where(i >= j, scores, 0.0).astype(BF16)
            o = dot(scores, vb[b, h])
            if b:
                scores = dot(qb[b, h], kb[0, h], ((1,), (1,))).astype(BF16)
                o += dot(scores, vb[0, h])
            lob[b, h] = o.astype(BF16)

    wq_copy.wait()
    queries(0)
    scan_b(0)
    wo_copy(1).wait()
    wo_send(1).start()
    queries(1)
    scan_b(1)
    for s in wg_copy:
        s.wait()
    gates(0, 0)
    scan_b(2)
    scan_b(3)

    @pl.when(z + 1 < nz)
    def _():
        pl.semaphore_wait(zsem, nz - 1 - z)

    scan_c(0)
    wo_copy(2).wait()
    wo_send(2).start()
    gates(1, 0)
    scan_c(1)
    gates(0, 1)
    scan_c(2)
    scan_c(3)
    scan_d(0)
    local(0)
    local(1)
    scan_d(1)
    wo_copy(3).wait()
    wo_send(3).start()
    gates(1, 1)
    scan_d(2)
    scan_d(3)
    local(2)
    local(3)

    def g_send(h):
        return remote(gsnd.at[h], gall.at[h, 1], gs_s.at[h], gs_r.at[h], {TP: other})

    def carried(h):
        start = pd[h].reshape(HEAD_K, HEAD_V)
        for own in (False, True):
            b = c if own else other
            o = lob[b, h].astype(F32) + dot(qb[b, h], start)
            scale = lax.rsqrt(jnp.mean(o * o, axis=-1, keepdims=True) + EPS)
            gated = (o * scale * gsb[b, h].astype(F32)).astype(BF16)
            if own:
                gall[h, 0] = gated
            else:
                gsnd[h] = gated

    def project(h, steps):
        gated = jnp.concatenate([gall[h, 0], gall[h, 1]], axis=1)
        for n in steps:
            at = slice(n * UNIT, (n + 1) * UNIT)
            part = dot(gated, wob[h, :, :, at].reshape(2 * HEAD_V, UNIT))
            if h:
                part += acc[n]
            if h < heads - 1:
                acc[n] = part
            else:
                out[:, at] = part.astype(BF16)

    first, rest = range(0, model // UNIT // 2), range(model // UNIT // 2, model // UNIT)

    def arrived(h):
        g_send(h).wait_recv()
        wo_send(h).wait_recv()

    scan_end(0)
    carried(0)
    g_send(0).start()
    scan_end(1)
    carried(1)
    g_send(1).start()
    for h in range(2, heads):
        scan_end(h)
        arrived(h - 2)
        carried(h)
        project(h - 2, first)
        g_send(h).start()
        project(h - 2, rest)
    for h in range(heads - 2, heads):
        arrived(h)
        project(h, first)
        project(h, rest)

    for i in range(token_steps):
        x_send(i).wait_send()
    for h in range(heads):
        wo_send(h).wait_send()
        g_send(h).wait_send()
        for d in range(1, nx):
            a_send(h, d).wait_send()
            d_send(h, d).wait_send()
        for d in range(1, ny):
            b_send(h, d).wait_send()
        for d in range(1, nz):

            @pl.when(z + d < nz)
            def _():
                c_send(h, d).wait_send()


def on_device(sizes, tok, gain, wq, wk, wv, wg, bias, hgain, wo):
    nz, ny, nx = sizes
    rows, width = tok.shape
    key_width, value_width, model = wq.shape[1], wv.shape[1], wo.shape[1]
    heads = key_width // HEAD_K
    pairs = heads // 2
    token_steps = 4
    most = max(sizes) - 1
    vmem = pltpu.VMEM
    dma = pltpu.SemaphoreType.DMA
    quarter = (HEAD_K // nx, HEAD_V)
    scratch = [
        vmem((2, rows, width), BF16),
        vmem((width, key_width), BF16),
        vmem((pairs, width, 2 * HEAD_V), BF16),
        vmem((width, key_width), BF16),
        vmem((pairs, width, 2 * HEAD_V), BF16),
        vmem((heads, 2, HEAD_V, model), BF16),
        vmem((1, width), F32),
        vmem((1, key_width), F32),
        vmem((1, value_width), F32),
        vmem((2, heads, rows, HEAD_K), BF16),
        vmem((2, heads, rows, HEAD_K), BF16),
        vmem((2, heads, rows, HEAD_V), BF16),
        vmem((2, heads, rows, HEAD_V), BF16),
        vmem((2, heads, rows, HEAD_V), BF16),
        vmem((model // UNIT, rows, UNIT), F32),
        vmem((heads, nx, *quarter), BF16),
        vmem((heads, nx, *quarter), BF16),
        vmem((heads, *quarter), BF16),
        vmem((heads, ny, *quarter), BF16),
        vmem((heads, *quarter), F32),
        vmem((heads, *quarter), BF16),
        vmem((heads, nz - 1, *quarter), BF16),
        vmem((heads, nx, *quarter), BF16),
        vmem((heads, nx, *quarter), BF16),
        vmem((heads, 2, rows, HEAD_V), BF16),
        vmem((heads, rows, HEAD_V), BF16),
        dma((token_steps,)),
        dma((3,)),
        dma((1,)),
        dma((pairs,)),
        dma((1,)),
        dma((pairs,)),
        dma((heads,)),
        dma((token_steps,)),
        dma((token_steps,)),
        dma((heads,)),
        dma((heads,)),
        dma((heads,)),
        dma((heads,)),
        dma((4, heads, most)),
        dma((4, heads, most)),
        pltpu.SemaphoreType.REGULAR,
    ]
    hbm = pl.BlockSpec(memory_space=pl.ANY)
    return pl.pallas_call(
        functools.partial(mixer, sizes),
        out_shape=pltpu.VMEM((rows, model), BF16),
        in_specs=[hbm] * 9,
        out_specs=pl.BlockSpec(memory_space=pltpu.VMEM),
        scratch_shapes=scratch,
        compiler_params=pltpu.CompilerParams(
            collective_id=0, has_side_effects=True, vmem_limit_bytes=64_500_000
        ),
        name="mixer",
    )(
        tok, gain.reshape(1, -1), wq, wk, wv, wg, bias.reshape(1, -1), hgain.reshape(1, -1), wo
    )


def solution(mesh, sizes=(4, 4, 4)):
    finer = Mesh(mesh.devices.reshape(*sizes, mesh.shape["tp"]), SP_TP)
    in_specs = (
        P(SP_TP, None),
        P(),
        P(None, "tp"),
        P(None, "tp"),
        P(None, "tp"),
        P(None, "tp"),
        P("tp"),
        P("tp"),
        P("tp", None),
    )
    return jax.shard_map(
        functools.partial(on_device, sizes),
        mesh=finer,
        in_specs=in_specs,
        out_specs=P(SP_TP, None),
        check_vma=False,
    )
```

```python
import functools
import math

import jax
import jax.numpy as jnp
from jax import lax
from jax.experimental import pallas as pl
from jax.experimental.pallas import tpu as pltpu
from jax.sharding import Mesh
from jax.sharding import PartitionSpec as P

HEAD_K = 128
HEAD_V = 256
Z, Y, X, TP = "sp_0", "sp_1", "sp_2", "tp"
SP_TP = (Z, Y, X, TP)
MESH = pl.DeviceIdType.MESH
UNIT = 512
EPS = 1e-06
DECAY_POWER = 16.0
F32, BF16 = jnp.float32, jnp.bfloat16


def remote(src, dst, send, recv, where):
    return pltpu.make_async_remote_copy(
        src_ref=src, dst_ref=dst, send_sem=send, recv_sem=recv, device_id=where, device_id_type=MESH
    )


def dot(a, b, dims=((1,), (0,))):
    return lax.dot_general(a, b, (dims, ((), ())), preferred_element_type=F32)


def mixer(
    sizes,
    tok, gain, wq, wk, wv, wg, bias, hgain, wo,
    out,
    xn, wkb, wvb, wqb, wgb, wob, gainb, biasb, hgainb,
    kb, qb, vb, gsb, lob, acc,
    sa, ra, tb, rb, yp, tc, rc, dd, pd,
    gall, gsnd,
    tok_sem, small_sem, k_sem, v_sem, q_sem, g_sem, wo_sem,
    xs, xr, ps, pr, gs_s, gs_r, scan_s, scan_r, line_sem,
):
    nz, ny, nx = sizes
    rows, width = xn.shape[1], xn.shape[2]
    heads = kb.shape[1]
    pairs = heads // 2
    chunk = HEAD_K // nx
    token_steps = tok_sem.shape[0]
    step_rows = rows // token_steps
    model = out.shape[1]
    z, y, x, c = (lax.axis_index(a) for a in SP_TP)
    other = 1 - c
    chip = (z * ny + y) * nx + x
    seq = nz * ny * nx * 2 * rows

    def token_copy(i):
        r = pl.ds(i * step_rows, step_rows)
        return pltpu.make_async_copy(tok.at[r, :], xn.at[c, r, :], tok_sem.at[i])

    small = [(gain, gainb), (bias, biasb), (hgain, hgainb)]
    small = [pltpu.make_async_copy(a, b, small_sem.at[i]) for i, (a, b) in enumerate(small)]
    v2 = 2 * HEAD_V
    wk_copy = pltpu.make_async_copy(wk, wkb, k_sem.at[0])
    wv_copy = [pltpu.make_async_copy(wv.at[:, pl.ds(p * v2, v2)], wvb.at[p], v_sem.at[p]) for p in range(pairs)]
    wq_copy = pltpu.make_async_copy(wq, wqb, q_sem.at[0])
    wg_copy = [pltpu.make_async_copy(wg.at[:, pl.ds(p * v2, v2)], wgb.at[p], g_sem.at[p]) for p in range(pairs)]

    def wo_copy(h):
        return pltpu.make_async_copy(wo.at[pl.ds(h * HEAD_V, HEAD_V), :], wob.at[h, 0], wo_sem.at[h])

    def wo_send(h):
        return remote(wob.at[h, 0], wob.at[h, 1], ps.at[h], pr.at[h], {TP: other})

    for s in small:
        s.start()
    for i in range(token_steps):
        token_copy(i).start()
    wk_copy.start(priority=1)

    barrier = pltpu.get_barrier_semaphore()
    lines = [(X, x, nx), (Y, y, ny), (Z, z, nz)]
    pl.semaphore_signal(barrier, inc=1, device_id={TP: other}, device_id_type=MESH)
    for axis, at, n in lines:
        for d in range(1, n):

            @pl.when(at + d < n)
            def _():
                pl.semaphore_signal(barrier, inc=1, device_id={axis: lax.rem(at + d, n)}, device_id_type=MESH)

    def tell_earlier():
        for i, (axis, at, n) in enumerate(lines):
            for d in range(1, n):

                @pl.when(at >= d)
                def _():
                    to = {axis: lax.rem(at - d + n, n)}
                    pl.semaphore_signal(line_sem.at[i], inc=1, device_id=to, device_id_type=MESH)

    def later_are_in(i):
        _, at, n = lines[i]

        @pl.when(at + 1 < n)
        def _():
            pl.semaphore_wait(line_sem.at[i], n - 1 - at)

    def x_send(i):
        r = pl.ds(i * step_rows, step_rows)
        return remote(xn.at[c, r, :], xn.at[c, r, :], xs.at[i], xr.at[i], {TP: other})

    def x_recv(i):
        r = pl.ds(i * step_rows, step_rows)
        return remote(xn.at[other, r, :], xn.at[other, r, :], xs.at[i], xr.at[i], {TP: other})

    for s in small:
        s.wait()
    for i in range(token_steps):
        token_copy(i).wait()
        if i == 0:
            wv_copy[0].start(priority=1)
        if i == token_steps - 1:
            wv_copy[1].start(priority=1)

        for g in range(step_rows // 16):
            r = pl.ds(i * step_rows + g * 16, 16)
            v = xn[c, r, :].astype(F32)
            scale = lax.rsqrt(jnp.mean(v * v, axis=-1, keepdims=True) + EPS)
            v = xn[c, r, :].astype(F32)
            xn[c, r, :] = (v * scale * gainb[...]).astype(BF16)
        if i == 0:
            pl.semaphore_wait(barrier, 1 + x + y + z)
        x_send(i).start()


    tell_earlier()

    logits = biasb[...] + math.log(seq / 8.0)
    log_decay = (jnp.minimum(logits, 0.0) - jnp.log1p(jnp.exp(-jnp.abs(logits)))) / DECAY_POWER

    def level(b):
        row = lax.broadcasted_iota(jnp.int32, (rows, 1), 0)
        pos = (row + (chip * 2 + b) * rows + (1 - seq // 2)).astype(F32)
        return pos * log_decay

    def scan_copy(phase, h, d, src, dst, axis, at, n):
        to = lax.rem(at + d, n)
        return remote(src, dst, scan_s.at[phase, h, d - 1], scan_r.at[phase, h, d - 1], {axis: to})

    def a_send(h, d):
        return scan_copy(0, h, d, sa.at[h, lax.rem(x + d, nx)], ra.at[h, x], X, x, nx)

    def a_recv(h, d):
        at = lax.rem(x + nx - d, nx)
        return scan_copy(0, h, d, sa.at[h, at], ra.at[h, at], X, x, nx)

    def b_send(h, d):
        return scan_copy(1, h, d, tb.at[h], rb.at[h, d - 1], Y, y, ny)

    def b_recv(h, d):
        return scan_copy(1, h, d, tb.at[h], rb.at[h, d - 1], Y, y, ny)

    def c_send(h, d):
        return scan_copy(2, h, d, tc.at[h], rc.at[h, d - 1], Z, z, nz)

    def c_recv(h, d):
        return scan_copy(2, h, d, tc.at[h], rc.at[h, d - 1], Z, z, nz)

    def d_send(h, d):
        return scan_copy(3, h, d, dd.at[h, lax.rem(x + d, nx)], pd.at[h, x], X, x, nx)

    def d_recv(h, d):
        at = lax.rem(x + nx - d, nx)
        return scan_copy(3, h, d, dd.at[h, at], pd.at[h, at], X, x, nx)

    far_first = lambda n: [2, 1, 3] if n == 4 else list(range(1, n))

    def scan_a(pair):
        for h in pair:
            k = kb[:, h].reshape(2 * rows, HEAD_K)
            v = vb[:, h].reshape(2 * rows, HEAD_V)
            sa[h] = dot(k, v, ((0,), (0,))).astype(BF16).reshape(nx, chunk, HEAD_V)
        for h in pair:
            for d in far_first(nx):
                a_send(h, d).start()
        for h in pair:
            ra[h, x] = sa[h, x]

    def scan_b(h):
        for d in range(1, nx):
            a_recv(h, d).wait_recv()
        total = ra[h, 0].astype(F32)
        for i in range(1, nx):
            total += ra[h, i].astype(F32)
        tb[h] = total.astype(BF16)
        for d in far_first(ny):
            b_send(h, d).start()

        @pl.when(y == 0)
        def _():
            yp[h] = jnp.zeros(yp.shape[1:], F32)

            @pl.when(z == 0)
            def _():
                scan_back(h)

    def scan_low(h):
        @pl.when(y > 0)
        def _():
            for d in range(1, ny):

                @pl.when(y >= d)
                def _():
                    b_recv(h, d).wait_recv()
                    part = rb[h, d - 1].astype(F32)
                    yp[h] = part if d == 1 else yp[h] + part

            @pl.when(z == 0)
            def _():
                scan_back(h)

    def scan_all(h):
        for d in range(1, ny):

            @pl.when(y < d)
            def _():
                b_recv(h, d).wait_recv()

        total = tb[h].astype(F32)
        for d in range(1, ny):
            total += rb[h, d - 1].astype(F32)
        tc[h] = total.astype(BF16)
        for d in far_first(nz):

            @pl.when(z + d < nz)
            def _():
                c_send(h, d).start()

    def scan_d(h):
        @pl.when(z > 0)
        def _():
            scan_z(h)
            scan_back(h)

    def scan_z(h):
        for d in range(1, nz):

            @pl.when(z >= d)
            def _():
                c_recv(h, d).wait_recv()
                yp[h] += rc[h, d - 1].astype(F32)

    def scan_back(h):
        before = yp[h]
        for i in range(nx):
            dd[h, i] = before.astype(BF16)
            before += ra[h, i].astype(F32)
        for d in far_first(nx):
            d_send(h, d).start()
        pd[h, x] = dd[h, x]

    def scan_end(h):
        for d in range(1, nx):
            d_recv(h, d).wait_recv()

    def keys(b):
        k = dot(xn[b], wkb[...]) * jnp.exp(-level(b))
        for h in range(heads):
            kb[b, h] = k[:, h * HEAD_K : (h + 1) * HEAD_K].astype(BF16)

    def values(b, p):
        v = dot(xn[b], wvb[p]).astype(BF16)
        for i in range(2):
            vb[b, 2 * p + i] = v[:, i * HEAD_V : (i + 1) * HEAD_V]

    wk_copy.wait()
    keys(c)
    wv_copy[0].wait()
    for h in range(heads):
        wo_copy(h).start(priority=1)
    values(c, 0)
    wq_copy.start(priority=1)
    for s in wg_copy:
        s.start(priority=1)
    for i in range(token_steps):
        x_recv(i).wait_recv()
    keys(other)
    values(other, 0)
    later_are_in(0)
    scan_a((0, 1))
    wv_copy[1].wait()
    wo_copy(0).wait()
    wo_send(0).start()
    values(c, 1)
    values(other, 1)
    scan_a((2, 3))

    def queries(b):
        q = dot(xn[b], wqb[...]) * (jnp.exp(level(b)) * HEAD_K**-0.5)
        for h in range(heads):
            qb[b, h] = q[:, h * HEAD_K : (h + 1) * HEAD_K].astype(BF16)

    def gates(b, p):
        u = dot(xn[b], wgb[p])
        u = u / (1.0 + jnp.exp(-u)) * hgainb[:, p * v2 : (p + 1) * v2]
        for i in range(2):
            gsb[b, 2 * p + i] = u[:, i * HEAD_V : (i + 1) * HEAD_V].astype(BF16)

    def local(h):
        i = lax.broadcasted_iota(jnp.int32, (rows, rows), 0)
        j = lax.broadcasted_iota(jnp.int32, (rows, rows), 1)
        for b in range(2):
            scores = dot(qb[b, h], kb[b, h], ((1,), (1,)))
            scores = jnp.where(i >= j, scores, 0.0).astype(BF16)
            o = dot(scores, vb[b, h])
            if b:
                scores = dot(qb[b, h], kb[0, h], ((1,), (1,))).astype(BF16)
                o += dot(scores, vb[0, h])
            lob[b, h] = o.astype(BF16)

    wq_copy.wait()
    queries(0)
    later_are_in(1)
    scan_b(0)
    wo_copy(1).wait()
    wo_send(1).start()
    queries(1)
    scan_b(1)
    for s in wg_copy:
        s.wait()
    gates(0, 0)
    scan_b(2)
    scan_b(3)
    wo_copy(2).wait()
    wo_send(2).start()
    gates(1, 0)
    scan_low(0)
    scan_low(1)
    later_are_in(2)

    @pl.when(y > 0)
    def _():
        scan_all(0)
        scan_all(1)

    gates(0, 1)

    @pl.when(y == 0)
    def _():
        scan_all(0)
        scan_all(1)

    local(0)
    scan_low(2)
    scan_low(3)

    @pl.when(y > 0)
    def _():
        scan_all(2)
        scan_all(3)


    @pl.when(y > 0)
    def _():
        scan_d(0)
        scan_d(1)

    local(1)

    @pl.when((y == 0) & (c == 0))
    def _():
        scan_all(2)
        scan_all(3)

    @pl.when(y == 0)
    def _():
        scan_d(0)
        scan_d(1)


    @pl.when((y == 0) & (c == 1))
    def _():
        scan_all(2)
        scan_all(3)

    wo_copy(3).wait()
    wo_send(3).start()
    gates(1, 1)
    scan_d(2)
    scan_d(3)

    def g_send(h):
        return remote(gsnd.at[h], gall.at[h, 1], gs_s.at[h], gs_r.at[h], {TP: other})

    def carried(h):
        start = pd[h].reshape(HEAD_K, HEAD_V)
        for own in (False, True):
            b = c if own else other
            o = lob[b, h].astype(F32) + dot(qb[b, h], start)
            scale = lax.rsqrt(jnp.mean(o * o, axis=-1, keepdims=True) + EPS)
            gated = (o * scale * gsb[b, h].astype(F32)).astype(BF16)
            if own:
                gall[h, 0] = gated
            else:
                gsnd[h] = gated

    def project(h, steps):
        gated = jnp.concatenate([gall[h, 0], gall[h, 1]], axis=1)
        for n in steps:
            at = slice(n * UNIT, (n + 1) * UNIT)
            part = dot(gated, wob[h, :, :, at].reshape(2 * HEAD_V, UNIT))
            if h:
                part += acc[n]
            if h < heads - 1:
                acc[n] = part
            else:
                out[:, at] = part.astype(BF16)

    first, rest = range(0, model // UNIT // 2), range(model // UNIT // 2, model // UNIT)

    def arrived(h):
        g_send(h).wait_recv()
        wo_send(h).wait_recv()

    scan_end(0)
    carried(0)
    g_send(0).start()
    scan_end(1)
    carried(1)
    g_send(1).start()
    local(2)
    local(3)
    scan_end(2)
    carried(2)
    g_send(2).start()
    scan_end(3)
    arrived(0)
    carried(3)
    project(0, first)
    g_send(3).start()
    project(0, rest)
    for h in range(1, heads):
        arrived(h)
        project(h, first)
        project(h, rest)

    for i in range(token_steps):
        x_send(i).wait_send()
    for h in range(heads):
        wo_send(h).wait_send()
        g_send(h).wait_send()
        for d in range(1, nx):
            a_send(h, d).wait_send()
            d_send(h, d).wait_send()
        for d in range(1, ny):
            b_send(h, d).wait_send()
        for d in range(1, nz):

            @pl.when(z + d < nz)
            def _():
                c_send(h, d).wait_send()


def on_device(sizes, tok, gain, wq, wk, wv, wg, bias, hgain, wo):
    nz, ny, nx = sizes
    rows, width = tok.shape
    key_width, value_width, model = wq.shape[1], wv.shape[1], wo.shape[1]
    heads = key_width // HEAD_K
    pairs = heads // 2
    token_steps = 4
    most = max(sizes) - 1
    vmem = pltpu.VMEM
    dma = pltpu.SemaphoreType.DMA
    quarter = (HEAD_K // nx, HEAD_V)
    scratch = [
        vmem((2, rows, width), BF16),
        vmem((width, key_width), BF16),
        vmem((pairs, width, 2 * HEAD_V), BF16),
        vmem((width, key_width), BF16),
        vmem((pairs, width, 2 * HEAD_V), BF16),
        vmem((heads, 2, HEAD_V, model), BF16),
        vmem((1, width), F32),
        vmem((1, key_width), F32),
        vmem((1, value_width), F32),
        vmem((2, heads, rows, HEAD_K), BF16),
        vmem((2, heads, rows, HEAD_K), BF16),
        vmem((2, heads, rows, HEAD_V), BF16),
        vmem((2, heads, rows, HEAD_V), BF16),
        vmem((2, heads, rows, HEAD_V), BF16),
        vmem((model // UNIT, rows, UNIT), F32),
        vmem((heads, nx, *quarter), BF16),
        vmem((heads, nx, *quarter), BF16),
        vmem((heads, *quarter), BF16),
        vmem((heads, ny - 1, *quarter), BF16),
        vmem((heads, *quarter), F32),
        vmem((heads, *quarter), BF16),
        vmem((heads, nz - 1, *quarter), BF16),
        vmem((heads, nx, *quarter), BF16),
        vmem((heads, nx, *quarter), BF16),
        vmem((heads, 2, rows, HEAD_V), BF16),
        vmem((heads, rows, HEAD_V), BF16),
        dma((token_steps,)),
        dma((3,)),
        dma((1,)),
        dma((pairs,)),
        dma((1,)),
        dma((pairs,)),
        dma((heads,)),
        dma((token_steps,)),
        dma((token_steps,)),
        dma((heads,)),
        dma((heads,)),
        dma((heads,)),
        dma((heads,)),
        dma((4, heads, most)),
        dma((4, heads, most)),
        pltpu.SemaphoreType.REGULAR((3,)),
    ]
    hbm = pl.BlockSpec(memory_space=pl.ANY)
    return pl.pallas_call(
        functools.partial(mixer, sizes),
        out_shape=pltpu.VMEM((rows, model), BF16),
        in_specs=[hbm] * 9,
        out_specs=pl.BlockSpec(memory_space=pltpu.VMEM),
        scratch_shapes=scratch,
        compiler_params=pltpu.CompilerParams(
            collective_id=0, has_side_effects=True, vmem_limit_bytes=64_500_000
        ),
        name="mixer",
    )(
        tok, gain.reshape(1, -1), wq, wk, wv, wg, bias.reshape(1, -1), hgain.reshape(1, -1), wo
    )


def solution(mesh, sizes=(4, 4, 4)):
    finer = Mesh(mesh.devices.reshape(*sizes, mesh.shape["tp"]), SP_TP)
    in_specs = (
        P(SP_TP, None),
        P(),
        P(None, "tp"),
        P(None, "tp"),
        P(None, "tp"),
        P(None, "tp"),
        P("tp"),
        P("tp"),
        P("tp", None),
    )
    return jax.shard_map(
        functools.partial(on_device, sizes),
        mesh=finer,
        in_specs=in_specs,
        out_specs=P(SP_TP, None),
        check_vma=False,
    )
```

```python
import functools
import math

import jax
import jax.numpy as jnp
from jax import lax
from jax.experimental import pallas as pl
from jax.experimental.pallas import tpu as pltpu
from jax.sharding import Mesh
from jax.sharding import PartitionSpec as P

HEAD_K = 128
HEAD_V = 256
Z, Y, X, TP = "sp_0", "sp_1", "sp_2", "tp"
SP_TP = (Z, Y, X, TP)
MESH = pl.DeviceIdType.MESH
UNIT = 512
EPS = 1e-06
DECAY_POWER = 16.0
F32, BF16 = jnp.float32, jnp.bfloat16


def remote(src, dst, send, recv, where):
    return pltpu.make_async_remote_copy(
        src_ref=src, dst_ref=dst, send_sem=send, recv_sem=recv, device_id=where, device_id_type=MESH
    )


def dot(a, b, dims=((1,), (0,))):
    return lax.dot_general(a, b, (dims, ((), ())), preferred_element_type=F32)


def mixer(
    sizes,
    tok, gain, wq, wk, wv, wg, bias, hgain, wo,
    acc, gall, wob,
    xn, wkb, wvb, wqb, wgb, wfirst, gainb, biasb, hgainb,
    kb, qb, vb, gsb, lob,
    sa, ra, tb, rb, yp, tc, rc, dd, pd,
    gfirst, gsnd,
    tok_sem, small_sem, k_sem, v_sem, q_sem, g_sem, wo_sem,
    xs, xr, ps, pr, gs_s, gs_r, scan_s, scan_r, line_sem,
):
    nz, ny, nx = sizes
    rows, width = xn.shape[1], xn.shape[2]
    heads = kb.shape[1]
    pairs = heads // 2
    chunk = HEAD_K // nx
    token_steps = tok_sem.shape[0]
    step_rows = rows // token_steps
    model = acc.shape[1]
    wpart = lambda h, i: wob.at[h - 2, i] if h > 1 else wfirst.at[i, h]
    gpart = lambda h, i: gall.at[h - 2, i] if h > 1 else gfirst.at[i, h]
    z, y, x, c = (lax.axis_index(a) for a in SP_TP)
    other = 1 - c
    chip = (z * ny + y) * nx + x
    seq = nz * ny * nx * 2 * rows

    def token_copy(i):
        r = pl.ds(i * step_rows, step_rows)
        return pltpu.make_async_copy(tok.at[r, :], xn.at[c, r, :], tok_sem.at[i])

    small = [(gain, gainb), (bias, biasb), (hgain, hgainb)]
    small = [pltpu.make_async_copy(a, b, small_sem.at[i]) for i, (a, b) in enumerate(small)]
    v2 = 2 * HEAD_V
    wk_copy = pltpu.make_async_copy(wk, wkb, k_sem.at[0])
    wv_copy = [pltpu.make_async_copy(wv.at[:, pl.ds(p * v2, v2)], wvb.at[p], v_sem.at[p]) for p in range(pairs)]
    wq_copy = pltpu.make_async_copy(wq, wqb, q_sem.at[0])
    wg_copy = [pltpu.make_async_copy(wg.at[:, pl.ds(p * v2, v2)], wgb.at[p], g_sem.at[p]) for p in range(pairs)]

    def wo_copy(h):
        return pltpu.make_async_copy(wo.at[pl.ds(h * HEAD_V, HEAD_V), :], wpart(h, 0), wo_sem.at[h])

    def wo_send(h):
        return remote(wpart(h, 0), wpart(h, 1), ps.at[h], pr.at[h], {TP: other})

    for s in small:
        s.start()
    for i in range(token_steps):
        token_copy(i).start()
    wk_copy.start(priority=1)

    barrier = pltpu.get_barrier_semaphore()
    lines = [(X, x, nx), (Y, y, ny), (Z, z, nz)]
    pl.semaphore_signal(barrier, inc=1, device_id={TP: other}, device_id_type=MESH)
    for axis, at, n in lines:
        for d in range(1, n):

            @pl.when(at + d < n)
            def _():
                pl.semaphore_signal(barrier, inc=1, device_id={axis: lax.rem(at + d, n)}, device_id_type=MESH)

    def tell_earlier():
        for i, (axis, at, n) in enumerate(lines):
            for d in range(1, n):

                @pl.when(at >= d)
                def _():
                    to = {axis: lax.rem(at - d + n, n)}
                    pl.semaphore_signal(line_sem.at[i], inc=1, device_id=to, device_id_type=MESH)

    def later_are_in(i):
        _, at, n = lines[i]

        @pl.when(at + 1 < n)
        def _():
            pl.semaphore_wait(line_sem.at[i], n - 1 - at)

    def x_send(i):
        r = pl.ds(i * step_rows, step_rows)
        return remote(xn.at[c, r, :], xn.at[c, r, :], xs.at[i], xr.at[i], {TP: other})

    def x_recv(i):
        r = pl.ds(i * step_rows, step_rows)
        return remote(xn.at[other, r, :], xn.at[other, r, :], xs.at[i], xr.at[i], {TP: other})

    for s in small:
        s.wait()
    for i in range(token_steps):
        token_copy(i).wait()
        if i == 0:
            wv_copy[0].start(priority=1)
        if i == token_steps - 1:
            wv_copy[1].start(priority=1)

        for g in range(step_rows // 16):
            r = pl.ds(i * step_rows + g * 16, 16)
            v = xn[c, r, :].astype(F32)
            scale = lax.rsqrt(jnp.mean(v * v, axis=-1, keepdims=True) + EPS)
            v = xn[c, r, :].astype(F32)
            xn[c, r, :] = (v * scale * gainb[...]).astype(BF16)
        if i == 0:
            pl.semaphore_wait(barrier, 1 + x + y + z)
        x_send(i).start()


    tell_earlier()

    logits = biasb[...] + math.log(seq / 8.0)
    log_decay = (jnp.minimum(logits, 0.0) - jnp.log1p(jnp.exp(-jnp.abs(logits)))) / DECAY_POWER

    def level(b):
        row = lax.broadcasted_iota(jnp.int32, (rows, 1), 0)
        pos = (row + (chip * 2 + b) * rows + (1 - seq // 2)).astype(F32)
        return pos * log_decay

    def scan_copy(phase, h, d, src, dst, axis, at, n):
        to = lax.rem(at + d, n)
        return remote(src, dst, scan_s.at[phase, h, d - 1], scan_r.at[phase, h, d - 1], {axis: to})

    def a_send(h, d):
        return scan_copy(0, h, d, sa.at[h, lax.rem(x + d, nx)], ra.at[h, x], X, x, nx)

    def a_recv(h, d):
        at = lax.rem(x + nx - d, nx)
        return scan_copy(0, h, d, sa.at[h, at], ra.at[h, at], X, x, nx)

    def b_send(h, d):
        return scan_copy(1, h, d, tb.at[h], rb.at[h, d - 1], Y, y, ny)

    def b_recv(h, d):
        return scan_copy(1, h, d, tb.at[h], rb.at[h, d - 1], Y, y, ny)

    def c_send(h, d):
        return scan_copy(2, h, d, tc.at[h], rc.at[h, d - 1], Z, z, nz)

    def c_recv(h, d):
        return scan_copy(2, h, d, tc.at[h], rc.at[h, d - 1], Z, z, nz)

    def d_send(h, d):
        return scan_copy(3, h, d, dd.at[h, lax.rem(x + d, nx)], pd.at[h, x], X, x, nx)

    def d_recv(h, d):
        at = lax.rem(x + nx - d, nx)
        return scan_copy(3, h, d, dd.at[h, at], pd.at[h, at], X, x, nx)

    far_first = lambda n: [2, 1, 3] if n == 4 else list(range(1, n))

    def scan_a(pair):
        for h in pair:
            k = kb[:, h].reshape(2 * rows, HEAD_K)
            v = vb[:, h].reshape(2 * rows, HEAD_V)
            sa[h] = dot(k, v, ((0,), (0,))).astype(BF16).reshape(nx, chunk, HEAD_V)
        for h in pair:
            for d in far_first(nx):
                a_send(h, d).start()
        for h in pair:
            ra[h, x] = sa[h, x]

    def scan_b(h):
        for d in range(1, nx):
            a_recv(h, d).wait_recv()
        total = ra[h, 0].astype(F32)
        for i in range(1, nx):
            total += ra[h, i].astype(F32)
        tb[h] = total.astype(BF16)
        for d in far_first(ny):
            b_send(h, d).start()

        @pl.when(y == 0)
        def _():
            yp[h] = jnp.zeros(yp.shape[1:], F32)

            @pl.when(z == 0)
            def _():
                scan_back(h)

    def scan_low(h):
        @pl.when(y > 0)
        def _():
            for d in range(1, ny):

                @pl.when(y >= d)
                def _():
                    b_recv(h, d).wait_recv()
                    part = rb[h, d - 1].astype(F32)
                    yp[h] = part if d == 1 else yp[h] + part

            @pl.when(z == 0)
            def _():
                scan_back(h)

    def scan_all(h):
        for d in range(1, ny):

            @pl.when(y < d)
            def _():
                b_recv(h, d).wait_recv()

        total = tb[h].astype(F32)
        for d in range(1, ny):
            total += rb[h, d - 1].astype(F32)
        tc[h] = total.astype(BF16)
        for d in far_first(nz):

            @pl.when(z + d < nz)
            def _():
                c_send(h, d).start()

    def scan_d(h):
        @pl.when(z > 0)
        def _():
            scan_z(h)
            scan_back(h)

    def scan_z(h):
        for d in range(1, nz):

            @pl.when(z >= d)
            def _():
                c_recv(h, d).wait_recv()
                yp[h] += rc[h, d - 1].astype(F32)

    def scan_back(h):
        before = yp[h]
        for i in range(nx):
            dd[h, i] = before.astype(BF16)
            before += ra[h, i].astype(F32)
        for d in far_first(nx):
            d_send(h, d).start()
        pd[h, x] = dd[h, x]

    def scan_end(h):
        for d in range(1, nx):
            d_recv(h, d).wait_recv()

    def keys(b):
        k = dot(xn[b], wkb[...]) * jnp.exp(-level(b))
        for h in range(heads):
            kb[b, h] = k[:, h * HEAD_K : (h + 1) * HEAD_K].astype(BF16)

    def values(b, p):
        v = dot(xn[b], wvb[p]).astype(BF16)
        for i in range(2):
            vb[b, 2 * p + i] = v[:, i * HEAD_V : (i + 1) * HEAD_V]

    wk_copy.wait()
    keys(c)
    wv_copy[0].wait()
    for h in range(heads):
        wo_copy(h).start(priority=1)
    values(c, 0)
    wq_copy.start(priority=1)
    for s in wg_copy:
        s.start(priority=1)
    for i in range(token_steps):
        x_recv(i).wait_recv()
    keys(other)
    values(other, 0)
    later_are_in(0)
    scan_a((0, 1))
    wv_copy[1].wait()
    wo_copy(0).wait()
    wo_send(0).start()
    values(c, 1)
    values(other, 1)
    scan_a((2, 3))

    def queries(b):
        q = dot(xn[b], wqb[...]) * (jnp.exp(level(b)) * HEAD_K**-0.5)
        for h in range(heads):
            qb[b, h] = q[:, h * HEAD_K : (h + 1) * HEAD_K].astype(BF16)

    def gates(b, p):
        u = dot(xn[b], wgb[p])
        u = u / (1.0 + jnp.exp(-u)) * hgainb[:, p * v2 : (p + 1) * v2]
        for i in range(2):
            gsb[b, 2 * p + i] = u[:, i * HEAD_V : (i + 1) * HEAD_V].astype(BF16)

    def local(h):
        i = lax.broadcasted_iota(jnp.int32, (rows, rows), 0)
        j = lax.broadcasted_iota(jnp.int32, (rows, rows), 1)
        for b in range(2):
            scores = dot(qb[b, h], kb[b, h], ((1,), (1,)))
            scores = jnp.where(i >= j, scores, 0.0).astype(BF16)
            o = dot(scores, vb[b, h])
            if b:
                scores = dot(qb[b, h], kb[0, h], ((1,), (1,))).astype(BF16)
                o += dot(scores, vb[0, h])
            lob[b, h] = o.astype(BF16)

    wq_copy.wait()
    queries(0)
    later_are_in(1)
    scan_b(0)
    wo_copy(1).wait()
    wo_send(1).start()
    queries(1)
    scan_b(1)
    for s in wg_copy:
        s.wait()
    gates(0, 0)
    scan_b(2)
    scan_b(3)
    wo_copy(2).wait()
    wo_send(2).start()
    gates(1, 0)
    scan_low(0)
    scan_low(1)
    later_are_in(2)

    @pl.when(y > 0)
    def _():
        scan_all(0)
        scan_all(1)

    gates(0, 1)

    @pl.when(y == 0)
    def _():
        scan_all(0)
        scan_all(1)

    local(0)
    scan_low(2)
    scan_low(3)

    @pl.when(y > 0)
    def _():
        scan_all(2)
        scan_all(3)


    @pl.when(y > 0)
    def _():
        scan_d(0)
        scan_d(1)

    local(1)

    @pl.when((y == 0) & (c == 0))
    def _():
        scan_all(2)
        scan_all(3)

    @pl.when(y == 0)
    def _():
        scan_d(0)
        scan_d(1)


    @pl.when((y == 0) & (c == 1))
    def _():
        scan_all(2)
        scan_all(3)

    wo_copy(3).wait()
    wo_send(3).start()
    gates(1, 1)
    scan_d(2)
    scan_d(3)

    def g_send(h):
        return remote(gsnd.at[h], gpart(h, 1), gs_s.at[h], gs_r.at[h], {TP: other})

    def carried(pair):
        for own in (False, True):
            for h in pair:
                b = c if own else other
                start = pd[h].reshape(HEAD_K, HEAD_V)
                o = lob[b, h].astype(F32) + dot(qb[b, h], start)
                scale = lax.rsqrt(jnp.mean(o * o, axis=-1, keepdims=True) + EPS)
                gated = (o * scale * gsb[b, h].astype(F32)).astype(BF16)
                if own:
                    gpart(h, 0)[...] = gated
                else:
                    gsnd[h] = gated
        for h in pair:
            g_send(h).start()

    def project(i):
        gated = jnp.concatenate([gfirst[i, 0], gfirst[i, 1]], axis=1)
        for n in range(model // UNIT):
            at = slice(n * UNIT, (n + 1) * UNIT)
            part = dot(gated, wfirst[i, :, :, at].reshape(2 * HEAD_V, UNIT))
            acc[:, at] = acc[:, at] + part if i else part

    def arrived(h):
        g_send(h).wait_recv()
        wo_send(h).wait_recv()

    local(2)
    local(3)
    scan_end(0)
    scan_end(1)
    carried((0, 1))
    project(0)
    scan_end(2)
    scan_end(3)
    carried((2, 3))
    arrived(0)
    arrived(1)
    project(1)
    for h in range(2, heads):
        arrived(h)

    for i in range(token_steps):
        x_send(i).wait_send()
    for h in range(heads):
        wo_send(h).wait_send()
        g_send(h).wait_send()
        for d in range(1, nx):
            a_send(h, d).wait_send()
            d_send(h, d).wait_send()
        for d in range(1, ny):
            b_send(h, d).wait_send()
        for d in range(1, nz):

            @pl.when(z + d < nz)
            def _():
                c_send(h, d).wait_send()


def finish(acc, gated, weight, out, stage, sem):
    rows, model = acc.shape
    depth = weight.shape[0] * 2 * HEAD_V
    left = jnp.concatenate([gated[h, i] for h in range(weight.shape[0]) for i in range(2)], axis=1)
    copies = []
    for n in range(model // UNIT):
        at = slice(n * UNIT, (n + 1) * UNIT)
        right = weight[:, :, :, at].reshape(depth, UNIT)
        stage[n] = (acc[:, at] + dot(left, right)).astype(BF16)
        copies.append(pltpu.make_async_copy(stage.at[n], out.at[:, pl.ds(n * UNIT, UNIT)], sem.at[n]))
        copies[-1].start()
    for copy in copies:
        copy.wait()


def on_device(sizes, tok, gain, wq, wk, wv, wg, bias, hgain, wo):
    nz, ny, nx = sizes
    rows, width = tok.shape
    key_width, value_width, model = wq.shape[1], wv.shape[1], wo.shape[1]
    heads = key_width // HEAD_K
    pairs = heads // 2
    token_steps = 4
    most = max(sizes) - 1
    vmem = pltpu.VMEM
    dma = pltpu.SemaphoreType.DMA
    quarter = (HEAD_K // nx, HEAD_V)
    scratch = [
        vmem((2, rows, width), BF16),
        vmem((width, key_width), BF16),
        vmem((pairs, width, 2 * HEAD_V), BF16),
        vmem((width, key_width), BF16),
        vmem((pairs, width, 2 * HEAD_V), BF16),
        vmem((2, 2, HEAD_V, model), BF16),
        vmem((1, width), F32),
        vmem((1, key_width), F32),
        vmem((1, value_width), F32),
        vmem((2, heads, rows, HEAD_K), BF16),
        vmem((2, heads, rows, HEAD_K), BF16),
        vmem((2, heads, rows, HEAD_V), BF16),
        vmem((2, heads, rows, HEAD_V), BF16),
        vmem((2, heads, rows, HEAD_V), BF16),
        vmem((heads, nx, *quarter), BF16),
        vmem((heads, nx, *quarter), BF16),
        vmem((heads, *quarter), BF16),
        vmem((heads, ny - 1, *quarter), BF16),
        vmem((heads, *quarter), F32),
        vmem((heads, *quarter), BF16),
        vmem((heads, nz - 1, *quarter), BF16),
        vmem((heads, nx, *quarter), BF16),
        vmem((heads, nx, *quarter), BF16),
        vmem((2, 2, rows, HEAD_V), BF16),
        vmem((heads, rows, HEAD_V), BF16),
        dma((token_steps,)),
        dma((3,)),
        dma((1,)),
        dma((pairs,)),
        dma((1,)),
        dma((pairs,)),
        dma((heads,)),
        dma((token_steps,)),
        dma((token_steps,)),
        dma((heads,)),
        dma((heads,)),
        dma((heads,)),
        dma((heads,)),
        dma((4, heads, most)),
        dma((4, heads, most)),
        pltpu.SemaphoreType.REGULAR((3,)),
    ]
    hbm = pl.BlockSpec(memory_space=pl.ANY)
    in_vmem = pl.BlockSpec(memory_space=vmem)
    parts = pl.pallas_call(
        functools.partial(mixer, sizes),
        out_shape=(
            vmem((rows, model), F32),
            vmem((heads - 2, 2, rows, HEAD_V), BF16),
            vmem((heads - 2, 2, HEAD_V, model), BF16),
        ),
        in_specs=[hbm] * 9,
        out_specs=[in_vmem] * 3,
        scratch_shapes=scratch,
        compiler_params=pltpu.CompilerParams(
            collective_id=0, has_side_effects=True, vmem_limit_bytes=52_500_000
        ),
        name="mixer",
    )(
        tok, gain.reshape(1, -1), wq, wk, wv, wg, bias.reshape(1, -1), hgain.reshape(1, -1), wo
    )
    return pl.pallas_call(
        finish,
        out_shape=jax.ShapeDtypeStruct((rows, model), BF16),
        in_specs=[in_vmem] * 3,
        out_specs=hbm,
        scratch_shapes=[vmem((model // UNIT, rows, UNIT), BF16), dma((model // UNIT,))],
        compiler_params=pltpu.CompilerParams(vmem_limit_bytes=8_000_000),
        name="finish",
    )(*parts)


def solution(mesh, sizes=(4, 4, 4)):
    finer = Mesh(mesh.devices.reshape(*sizes, mesh.shape["tp"]), SP_TP)
    in_specs = (
        P(SP_TP, None),
        P(),
        P(None, "tp"),
        P(None, "tp"),
        P(None, "tp"),
        P(None, "tp"),
        P("tp"),
        P("tp"),
        P("tp", None),
    )
    return jax.shard_map(
        functools.partial(on_device, sizes),
        mesh=finer,
        in_specs=in_specs,
        out_specs=P(SP_TP, None),
        check_vma=False,
    )
```

```python
import functools
import math

import jax
import jax.numpy as jnp
from jax import lax
from jax.experimental import pallas as pl
from jax.experimental.pallas import tpu as pltpu
from jax.sharding import Mesh
from jax.sharding import PartitionSpec as P

HEAD_K = 128
HEAD_V = 256
Z, Y, X, TP = "sp_0", "sp_1", "sp_2", "tp"
SP_TP = (Z, Y, X, TP)
MESH = pl.DeviceIdType.MESH
UNIT = 512
EPS = 1e-06
DECAY_POWER = 16.0
F32, BF16 = jnp.float32, jnp.bfloat16


def remote(src, dst, send, recv, where):
    return pltpu.make_async_remote_copy(
        src_ref=src, dst_ref=dst, send_sem=send, recv_sem=recv, device_id=where, device_id_type=MESH
    )


def dot(a, b, dims=((1,), (0,))):
    return lax.dot_general(a, b, (dims, ((), ())), preferred_element_type=F32)


def mixer(
    sizes,
    tok, gain, wq, wk, wv, wg, bias, hgain, wo,
    acc, gall, wob,
    xn, wkb, wvb, wqb, wgb, wfirst, gainb, biasb, hgainb,
    kb, qb, vb, gsb, lob,
    sa, ra, tb, rb, yp, tc, rc, dd, pd,
    gfirst, gsnd,
    tok_sem, small_sem, k_sem, v_sem, q_sem, g_sem, wo_sem,
    xs, xr, ps, pr, gs_s, gs_r, scan_s, scan_r, line_sem,
):
    nz, ny, nx = sizes
    rows, width = xn.shape[1], xn.shape[2]
    heads = kb.shape[1]
    pairs = heads // 2
    chunk = HEAD_K // nx
    token_steps = tok_sem.shape[0]
    step_rows = rows // token_steps
    model = acc.shape[1]

    def part_of(first, last, h, i):
        if i and h > 1:
            return last.at[h - 2]
        return first.at[2 if i else h // 2, h % 2]

    wpart = functools.partial(part_of, wfirst, wob)
    gpart = functools.partial(part_of, gfirst, gall)
    z, y, x, c = (lax.axis_index(a) for a in SP_TP)
    other = 1 - c
    chip = (z * ny + y) * nx + x
    seq = nz * ny * nx * 2 * rows

    def token_copy(i):
        r = pl.ds(i * step_rows, step_rows)
        return pltpu.make_async_copy(tok.at[r, :], xn.at[c, r, :], tok_sem.at[i])

    small = [(gain, gainb), (bias, biasb), (hgain, hgainb)]
    small = [pltpu.make_async_copy(a, b, small_sem.at[i]) for i, (a, b) in enumerate(small)]
    v2 = 2 * HEAD_V
    wk_copy = pltpu.make_async_copy(wk, wkb, k_sem.at[0])
    wv_copy = [pltpu.make_async_copy(wv.at[:, pl.ds(p * v2, v2)], wvb.at[p], v_sem.at[p]) for p in range(pairs)]
    wq_copy = pltpu.make_async_copy(wq, wqb, q_sem.at[0])
    wg_copy = [pltpu.make_async_copy(wg.at[:, pl.ds(p * v2, v2)], wgb.at[p], g_sem.at[p]) for p in range(pairs)]

    def wo_copy(h):
        return pltpu.make_async_copy(wo.at[pl.ds(h * HEAD_V, HEAD_V), :], wpart(h, 0), wo_sem.at[h])

    def wo_send(h):
        return remote(wpart(h, 0), wpart(h, 1), ps.at[h], pr.at[h], {TP: other})

    for s in small:
        s.start()
    for i in range(token_steps):
        token_copy(i).start()
    wk_copy.start(priority=1)

    barrier = pltpu.get_barrier_semaphore()
    lines = [(X, x, nx), (Y, y, ny), (Z, z, nz)]
    pl.semaphore_signal(barrier, inc=1, device_id={TP: other}, device_id_type=MESH)
    for axis, at, n in lines:
        for d in range(1, n):

            @pl.when(at + d < n)
            def _():
                pl.semaphore_signal(barrier, inc=1, device_id={axis: lax.rem(at + d, n)}, device_id_type=MESH)

    def tell_earlier():
        for i, (axis, at, n) in enumerate(lines):
            for d in range(1, n):

                @pl.when(at >= d)
                def _():
                    to = {axis: lax.rem(at - d + n, n)}
                    pl.semaphore_signal(line_sem.at[i], inc=1, device_id=to, device_id_type=MESH)

    def later_are_in(i):
        _, at, n = lines[i]

        @pl.when(at + 1 < n)
        def _():
            pl.semaphore_wait(line_sem.at[i], n - 1 - at)

    def x_send(i):
        r = pl.ds(i * step_rows, step_rows)
        return remote(xn.at[c, r, :], xn.at[c, r, :], xs.at[i], xr.at[i], {TP: other})

    def x_recv(i):
        r = pl.ds(i * step_rows, step_rows)
        return remote(xn.at[other, r, :], xn.at[other, r, :], xs.at[i], xr.at[i], {TP: other})

    for s in small:
        s.wait()
    for i in range(token_steps):
        token_copy(i).wait()
        if i == 0:
            wv_copy[0].start(priority=1)
        if i == token_steps - 1:
            wv_copy[1].start(priority=1)

        for g in range(step_rows // 16):
            r = pl.ds(i * step_rows + g * 16, 16)
            v = xn[c, r, :].astype(F32)
            scale = lax.rsqrt(jnp.mean(v * v, axis=-1, keepdims=True) + EPS)
            v = xn[c, r, :].astype(F32)
            xn[c, r, :] = (v * scale * gainb[...]).astype(BF16)
        if i == 0:
            pl.semaphore_wait(barrier, 1 + x + y + z)
        x_send(i).start()


    tell_earlier()

    logits = biasb[...] + math.log(seq / 8.0)
    log_decay = (jnp.minimum(logits, 0.0) - jnp.log1p(jnp.exp(-jnp.abs(logits)))) / DECAY_POWER

    def level(b):
        row = lax.broadcasted_iota(jnp.int32, (rows, 1), 0)
        pos = (row + (chip * 2 + b) * rows + (1 - seq // 2)).astype(F32)
        return pos * log_decay

    def scan_copy(phase, h, d, src, dst, axis, at, n):
        to = lax.rem(at + d, n)
        return remote(src, dst, scan_s.at[phase, h, d - 1], scan_r.at[phase, h, d - 1], {axis: to})

    def a_send(h, d):
        return scan_copy(0, h, d, sa.at[h, lax.rem(x + d, nx)], ra.at[h, x], X, x, nx)

    def a_recv(h, d):
        at = lax.rem(x + nx - d, nx)
        return scan_copy(0, h, d, sa.at[h, at], ra.at[h, at], X, x, nx)

    def b_send(h, d):
        return scan_copy(1, h, d, tb.at[h], rb.at[h, d - 1], Y, y, ny)

    def b_recv(h, d):
        return scan_copy(1, h, d, tb.at[h], rb.at[h, d - 1], Y, y, ny)

    def c_send(h, d):
        return scan_copy(2, h, d, tc.at[h], rc.at[h, d - 1], Z, z, nz)

    def c_recv(h, d):
        return scan_copy(2, h, d, tc.at[h], rc.at[h, d - 1], Z, z, nz)

    def d_send(h, d):
        return scan_copy(3, h, d, dd.at[h, lax.rem(x + d, nx)], pd.at[h, x], X, x, nx)

    def d_recv(h, d):
        at = lax.rem(x + nx - d, nx)
        return scan_copy(3, h, d, dd.at[h, at], pd.at[h, at], X, x, nx)

    far_first = lambda n: [2, 1, 3] if n == 4 else list(range(1, n))

    def scan_a(pair):
        for h in pair:
            k = kb[:, h].reshape(2 * rows, HEAD_K)
            v = vb[:, h].reshape(2 * rows, HEAD_V)
            sa[h] = dot(k, v, ((0,), (0,))).astype(BF16).reshape(nx, chunk, HEAD_V)
        for h in pair:
            for d in far_first(nx):
                a_send(h, d).start()
        for h in pair:
            ra[h, x] = sa[h, x]

    def scan_b(h):
        for d in range(1, nx):
            a_recv(h, d).wait_recv()
        total = ra[h, 0].astype(F32)
        for i in range(1, nx):
            total += ra[h, i].astype(F32)
        tb[h] = total.astype(BF16)
        for d in far_first(ny):
            b_send(h, d).start()

        @pl.when(y == 0)
        def _():
            yp[h] = jnp.zeros(yp.shape[1:], F32)

            @pl.when(z == 0)
            def _():
                scan_back(h)

    def scan_low(h):
        @pl.when(y > 0)
        def _():
            for d in range(1, ny):

                @pl.when(y >= d)
                def _():
                    b_recv(h, d).wait_recv()
                    part = rb[h, d - 1].astype(F32)
                    yp[h] = part if d == 1 else yp[h] + part

            @pl.when(z == 0)
            def _():
                scan_back(h)

    def scan_all(h):
        for d in range(1, ny):

            @pl.when(y < d)
            def _():
                b_recv(h, d).wait_recv()

        total = tb[h].astype(F32)
        for d in range(1, ny):
            total += rb[h, d - 1].astype(F32)
        tc[h] = total.astype(BF16)
        for d in far_first(nz):

            @pl.when(z + d < nz)
            def _():
                c_send(h, d).start()

    def scan_d(h):
        @pl.when(z > 0)
        def _():
            scan_z(h)
            scan_back(h)

    def scan_z(h):
        for d in range(1, nz):

            @pl.when(z >= d)
            def _():
                c_recv(h, d).wait_recv()
                yp[h] += rc[h, d - 1].astype(F32)

    def scan_back(h):
        before = yp[h]
        for i in range(nx):
            dd[h, i] = before.astype(BF16)
            before += ra[h, i].astype(F32)
        for d in far_first(nx):
            d_send(h, d).start()
        pd[h, x] = dd[h, x]

    def scan_end(h):
        for d in range(1, nx):
            d_recv(h, d).wait_recv()

    def keys(b):
        k = dot(xn[b], wkb[...]) * jnp.exp(-level(b))
        for h in range(heads):
            kb[b, h] = k[:, h * HEAD_K : (h + 1) * HEAD_K].astype(BF16)

    def values(b, p):
        v = dot(xn[b], wvb[p]).astype(BF16)
        for i in range(2):
            vb[b, 2 * p + i] = v[:, i * HEAD_V : (i + 1) * HEAD_V]

    wk_copy.wait()
    keys(c)
    wv_copy[0].wait()
    for h in range(heads):
        wo_copy(h).start(priority=1)
    values(c, 0)
    wq_copy.start(priority=1)
    for s in wg_copy:
        s.start(priority=1)
    for i in range(token_steps):
        x_recv(i).wait_recv()
    keys(other)
    values(other, 0)
    later_are_in(0)
    scan_a((0, 1))
    wv_copy[1].wait()
    wo_copy(0).wait()
    wo_send(0).start()
    values(c, 1)
    values(other, 1)
    scan_a((2, 3))

    def queries(b):
        q = dot(xn[b], wqb[...]) * (jnp.exp(level(b)) * HEAD_K**-0.5)
        for h in range(heads):
            qb[b, h] = q[:, h * HEAD_K : (h + 1) * HEAD_K].astype(BF16)

    def gates(b, p):
        u = dot(xn[b], wgb[p])
        u = u / (1.0 + jnp.exp(-u)) * hgainb[:, p * v2 : (p + 1) * v2]
        for i in range(2):
            gsb[b, 2 * p + i] = u[:, i * HEAD_V : (i + 1) * HEAD_V].astype(BF16)

    def local(h):
        i = lax.broadcasted_iota(jnp.int32, (rows, rows), 0)
        j = lax.broadcasted_iota(jnp.int32, (rows, rows), 1)
        for b in range(2):
            scores = dot(qb[b, h], kb[b, h], ((1,), (1,)))
            scores = jnp.where(i >= j, scores, 0.0).astype(BF16)
            o = dot(scores, vb[b, h])
            if b:
                scores = dot(qb[b, h], kb[0, h], ((1,), (1,))).astype(BF16)
                o += dot(scores, vb[0, h])
            lob[b, h] = o.astype(BF16)

    wq_copy.wait()
    queries(0)
    later_are_in(1)
    scan_b(0)
    wo_copy(1).wait()
    wo_send(1).start()
    queries(1)
    scan_b(1)
    for s in wg_copy:
        s.wait()
    gates(0, 0)
    scan_b(2)
    scan_b(3)
    wo_copy(2).wait()
    wo_send(2).start()
    gates(1, 0)
    scan_low(0)
    scan_low(1)
    later_are_in(2)

    @pl.when(y > 0)
    def _():
        scan_all(0)
        scan_all(1)

    gates(0, 1)

    @pl.when(y == 0)
    def _():
        scan_all(0)
        scan_all(1)

    local(0)
    scan_low(2)
    scan_low(3)

    @pl.when(y > 0)
    def _():
        scan_all(2)
        scan_all(3)


    @pl.when(y > 0)
    def _():
        scan_d(0)
        scan_d(1)

    local(1)

    @pl.when((y == 0) & (c == 0))
    def _():
        scan_all(2)
        scan_all(3)

    @pl.when(y == 0)
    def _():
        scan_d(0)
        scan_d(1)


    @pl.when((y == 0) & (c == 1))
    def _():
        scan_all(2)
        scan_all(3)

    wo_copy(3).wait()
    wo_send(3).start()
    gates(1, 1)
    scan_d(2)
    scan_d(3)

    def g_send(h):
        return remote(gsnd.at[h], gpart(h, 1), gs_s.at[h], gs_r.at[h], {TP: other})

    def carried(pair):
        for own in (False, True):
            for h in pair:
                b = c if own else other
                start = pd[h].reshape(HEAD_K, HEAD_V)
                o = lob[b, h].astype(F32) + dot(qb[b, h], start)
                scale = lax.rsqrt(jnp.mean(o * o, axis=-1, keepdims=True) + EPS)
                gated = (o * scale * gsb[b, h].astype(F32)).astype(BF16)
                if own:
                    gpart(h, 0)[...] = gated
                else:
                    gsnd[h] = gated
        for h in pair:
            g_send(h).start()

    def project(groups):
        lo, hi = groups[0], groups[-1] + 1
        gated = jnp.concatenate([gfirst[g, h] for g in groups for h in range(2)], axis=1)
        for n in range(model // UNIT):
            at = slice(n * UNIT, (n + 1) * UNIT)
            part = dot(gated, wfirst[lo:hi, :, :, at].reshape((hi - lo) * 2 * HEAD_V, UNIT))
            acc[:, at] = acc[:, at] + part if lo else part

    def arrived(h):
        g_send(h).wait_recv()
        wo_send(h).wait_recv()

    local(2)
    local(3)
    scan_end(0)
    scan_end(1)
    carried((0, 1))
    project((0,))
    scan_end(2)
    scan_end(3)
    carried((2, 3))

    @pl.when(c == 1)
    def _():
        project((1,))

    arrived(0)
    arrived(1)

    @pl.when(c == 1)
    def _():
        project((2,))

    @pl.when(c == 0)
    def _():
        project((1, 2))

    for h in range(2, heads):
        arrived(h)

    for i in range(token_steps):
        x_send(i).wait_send()
    for h in range(heads):
        wo_send(h).wait_send()
        g_send(h).wait_send()
        for d in range(1, nx):
            a_send(h, d).wait_send()
            d_send(h, d).wait_send()
        for d in range(1, ny):
            b_send(h, d).wait_send()
        for d in range(1, nz):

            @pl.when(z + d < nz)
            def _():
                c_send(h, d).wait_send()


def finish(acc, gated, weight, out, stage, sem):
    rows, model = acc.shape
    left = jnp.concatenate([gated[0], gated[1]], axis=1)
    copies = []
    for n in range(model // UNIT):
        at = slice(n * UNIT, (n + 1) * UNIT)
        right = weight[:, :, at].reshape(2 * HEAD_V, UNIT)
        stage[n] = (acc[:, at] + dot(left, right)).astype(BF16)
        copies.append(pltpu.make_async_copy(stage.at[n], out.at[:, pl.ds(n * UNIT, UNIT)], sem.at[n]))
        copies[-1].start()
    for copy in copies:
        copy.wait()


def on_device(sizes, tok, gain, wq, wk, wv, wg, bias, hgain, wo):
    nz, ny, nx = sizes
    rows, width = tok.shape
    key_width, value_width, model = wq.shape[1], wv.shape[1], wo.shape[1]
    heads = key_width // HEAD_K
    pairs = heads // 2
    token_steps = 4
    most = max(sizes) - 1
    vmem = pltpu.VMEM
    dma = pltpu.SemaphoreType.DMA
    quarter = (HEAD_K // nx, HEAD_V)
    scratch = [
        vmem((2, rows, width), BF16),
        vmem((width, key_width), BF16),
        vmem((pairs, width, 2 * HEAD_V), BF16),
        vmem((width, key_width), BF16),
        vmem((pairs, width, 2 * HEAD_V), BF16),
        vmem((3, 2, HEAD_V, model), BF16),
        vmem((1, width), F32),
        vmem((1, key_width), F32),
        vmem((1, value_width), F32),
        vmem((2, heads, rows, HEAD_K), BF16),
        vmem((2, heads, rows, HEAD_K), BF16),
        vmem((2, heads, rows, HEAD_V), BF16),
        vmem((2, heads, rows, HEAD_V), BF16),
        vmem((2, heads, rows, HEAD_V), BF16),
        vmem((heads, nx, *quarter), BF16),
        vmem((heads, nx, *quarter), BF16),
        vmem((heads, *quarter), BF16),
        vmem((heads, ny - 1, *quarter), BF16),
        vmem((heads, *quarter), F32),
        vmem((heads, *quarter), BF16),
        vmem((heads, nz - 1, *quarter), BF16),
        vmem((heads, nx, *quarter), BF16),
        vmem((heads, nx, *quarter), BF16),
        vmem((3, 2, rows, HEAD_V), BF16),
        vmem((heads, rows, HEAD_V), BF16),
        dma((token_steps,)),
        dma((3,)),
        dma((1,)),
        dma((pairs,)),
        dma((1,)),
        dma((pairs,)),
        dma((heads,)),
        dma((token_steps,)),
        dma((token_steps,)),
        dma((heads,)),
        dma((heads,)),
        dma((heads,)),
        dma((heads,)),
        dma((4, heads, most)),
        dma((4, heads, most)),
        pltpu.SemaphoreType.REGULAR((3,)),
    ]
    hbm = pl.BlockSpec(memory_space=pl.ANY)
    in_vmem = pl.BlockSpec(memory_space=vmem)
    parts = pl.pallas_call(
        functools.partial(mixer, sizes),
        out_shape=(
            vmem((rows, model), F32),
            vmem((2, rows, HEAD_V), BF16),
            vmem((2, HEAD_V, model), BF16),
        ),
        in_specs=[hbm] * 9,
        out_specs=[in_vmem] * 3,
        scratch_shapes=scratch,
        compiler_params=pltpu.CompilerParams(
            collective_id=0, has_side_effects=True, vmem_limit_bytes=57_000_000
        ),
        name="mixer",
    )(
        tok, gain.reshape(1, -1), wq, wk, wv, wg, bias.reshape(1, -1), hgain.reshape(1, -1), wo
    )
    return pl.pallas_call(
        finish,
        out_shape=jax.ShapeDtypeStruct((rows, model), BF16),
        in_specs=[in_vmem] * 3,
        out_specs=hbm,
        scratch_shapes=[vmem((model // UNIT, rows, UNIT), BF16), dma((model // UNIT,))],
        compiler_params=pltpu.CompilerParams(vmem_limit_bytes=8_000_000),
        name="finish",
    )(*parts)


def solution(mesh, sizes=(4, 4, 4)):
    finer = Mesh(mesh.devices.reshape(*sizes, mesh.shape["tp"]), SP_TP)
    in_specs = (
        P(SP_TP, None),
        P(),
        P(None, "tp"),
        P(None, "tp"),
        P(None, "tp"),
        P(None, "tp"),
        P("tp"),
        P("tp"),
        P("tp", None),
    )
    return jax.shard_map(
        functools.partial(on_device, sizes),
        mesh=finer,
        in_specs=in_specs,
        out_specs=P(SP_TP, None),
        check_vma=False,
    )
```

```python
import functools
import math

import jax
import jax.numpy as jnp
from jax import lax
from jax.experimental import pallas as pl
from jax.experimental.pallas import tpu as pltpu
from jax.sharding import Mesh
from jax.sharding import PartitionSpec as P

HEAD_K = 128
HEAD_V = 256
Z, Y, X, TP = "sp_0", "sp_1", "sp_2", "tp"
SP_TP = (Z, Y, X, TP)
MESH = pl.DeviceIdType.MESH
UNIT = 512
EPS = 1e-06
DECAY_POWER = 16.0
F32, BF16 = jnp.float32, jnp.bfloat16


def remote(src, dst, send, recv, where):
    return pltpu.make_async_remote_copy(
        src_ref=src, dst_ref=dst, send_sem=send, recv_sem=recv, device_id=where, device_id_type=MESH
    )


def dot(a, b, dims=((1,), (0,))):
    return lax.dot_general(a, b, (dims, ((), ())), preferred_element_type=F32)


def mixer(
    sizes,
    tok, gain, wq, wk, wv, wg, bias, hgain, wo,
    acc, gall, wob,
    xn, wkb, wvb, wqb, wgb, wfirst, gainb, biasb, hgainb,
    kb, qb, vb, gsb, lob,
    sa, ra, tb, rb, yp, tc, rc, dd, pd,
    gfirst, gsnd,
    tok_sem, small_sem, k_sem, v_sem, q_sem, g_sem, wo_sem,
    xs, xr, ps, pr, gs_s, gs_r, scan_s, scan_r, line_sem,
):
    nz, ny, nx = sizes
    rows, width = xn.shape[1], xn.shape[2]
    heads = kb.shape[1]
    pairs = heads // 2
    chunk = HEAD_K // nx
    token_steps = tok_sem.shape[0]
    step_rows = rows // token_steps
    model = acc.shape[1]
    wpart = lambda h, i: wob.at[h - 2, i] if h > 1 else wfirst.at[i, h]
    gpart = lambda h, i: gall.at[h - 2, i] if h > 1 else gfirst.at[i, h]
    z, y, x, c = (lax.axis_index(a) for a in SP_TP)
    other = 1 - c
    chip = (z * ny + y) * nx + x
    seq = nz * ny * nx * 2 * rows

    def token_copy(i):
        r = pl.ds(i * step_rows, step_rows)
        return pltpu.make_async_copy(tok.at[r, :], xn.at[c, r, :], tok_sem.at[i])

    small = [(gain, gainb), (bias, biasb), (hgain, hgainb)]
    small = [pltpu.make_async_copy(a, b, small_sem.at[i]) for i, (a, b) in enumerate(small)]
    v2 = 2 * HEAD_V
    step = width // k_sem.shape[0]
    wk_copy = [
        pltpu.make_async_copy(wk.at[pl.ds(i * step, step), :], wkb.at[pl.ds(i * step, step), :], k_sem.at[i])
        for i in range(k_sem.shape[0])
    ]
    wv_copy = [
        [
            pltpu.make_async_copy(
                wv.at[pl.ds(i * step, step), pl.ds(p * v2, v2)], wvb.at[p, pl.ds(i * step, step), :], v_sem.at[p, i]
            )
            for i in range(k_sem.shape[0])
        ]
        for p in range(pairs)
    ]
    wq_copy = pltpu.make_async_copy(wq, wqb, q_sem.at[0])
    wg_copy = [pltpu.make_async_copy(wg.at[:, pl.ds(p * v2, v2)], wgb.at[p], g_sem.at[p]) for p in range(pairs)]

    def wo_copy(h):
        return pltpu.make_async_copy(wo.at[pl.ds(h * HEAD_V, HEAD_V), :], wpart(h, 0), wo_sem.at[h])

    def wo_send(h):
        return remote(wpart(h, 0), wpart(h, 1), ps.at[h], pr.at[h], {TP: other})

    for s in small:
        s.start()
    for i in range(token_steps):
        token_copy(i).start()
    for s in wk_copy:
        s.start(priority=1)

    barrier = pltpu.get_barrier_semaphore()
    lines = [(X, x, nx), (Y, y, ny), (Z, z, nz)]
    pl.semaphore_signal(barrier, inc=1, device_id={TP: other}, device_id_type=MESH)
    for axis, at, n in lines:
        for d in range(1, n):

            @pl.when(at + d < n)
            def _():
                pl.semaphore_signal(barrier, inc=1, device_id={axis: lax.rem(at + d, n)}, device_id_type=MESH)

    def tell_earlier():
        for i, (axis, at, n) in enumerate(lines):
            for d in range(1, n):

                @pl.when(at >= d)
                def _():
                    to = {axis: lax.rem(at - d + n, n)}
                    pl.semaphore_signal(line_sem.at[i], inc=1, device_id=to, device_id_type=MESH)

    def later_are_in(i):
        _, at, n = lines[i]

        @pl.when(at + 1 < n)
        def _():
            pl.semaphore_wait(line_sem.at[i], n - 1 - at)

    def x_send(i):
        r = pl.ds(i * step_rows, step_rows)
        return remote(xn.at[c, r, :], xn.at[c, r, :], xs.at[i], xr.at[i], {TP: other})

    def x_recv(i):
        r = pl.ds(i * step_rows, step_rows)
        return remote(xn.at[other, r, :], xn.at[other, r, :], xs.at[i], xr.at[i], {TP: other})

    for s in small:
        s.wait()
    for i in range(token_steps):
        token_copy(i).wait()
        if i == 0:
            for s in wv_copy[0]:
                s.start(priority=1)
        if i == token_steps - 1:
            for s in wv_copy[1]:
                s.start(priority=1)

        for g in range(step_rows // 16):
            r = pl.ds(i * step_rows + g * 16, 16)
            v = xn[c, r, :].astype(F32)
            scale = lax.rsqrt(jnp.mean(v * v, axis=-1, keepdims=True) + EPS)
            v = xn[c, r, :].astype(F32)
            xn[c, r, :] = (v * scale * gainb[...]).astype(BF16)
        if i == 0:
            pl.semaphore_wait(barrier, 1 + x + y + z)
        x_send(i).start()


    tell_earlier()

    logits = biasb[...] + math.log(seq / 8.0)
    log_decay = (jnp.minimum(logits, 0.0) - jnp.log1p(jnp.exp(-jnp.abs(logits)))) / DECAY_POWER

    def level(b):
        row = lax.broadcasted_iota(jnp.int32, (rows, 1), 0)
        pos = (row + (chip * 2 + b) * rows + (1 - seq // 2)).astype(F32)
        return pos * log_decay

    def scan_copy(phase, h, d, src, dst, axis, at, n):
        to = lax.rem(at + d, n)
        return remote(src, dst, scan_s.at[phase, h, d - 1], scan_r.at[phase, h, d - 1], {axis: to})

    def a_send(h, d):
        return scan_copy(0, h, d, sa.at[h, lax.rem(x + d, nx)], ra.at[h, x], X, x, nx)

    def a_recv(h, d):
        at = lax.rem(x + nx - d, nx)
        return scan_copy(0, h, d, sa.at[h, at], ra.at[h, at], X, x, nx)

    def b_send(h, d):
        return scan_copy(1, h, d, tb.at[h], rb.at[h, d - 1], Y, y, ny)

    def b_recv(h, d):
        return scan_copy(1, h, d, tb.at[h], rb.at[h, d - 1], Y, y, ny)

    def c_send(h, d):
        return scan_copy(2, h, d, tc.at[h], rc.at[h, d - 1], Z, z, nz)

    def c_recv(h, d):
        return scan_copy(2, h, d, tc.at[h], rc.at[h, d - 1], Z, z, nz)

    def d_send(h, d):
        return scan_copy(3, h, d, dd.at[h, lax.rem(x + d, nx)], pd.at[h, x], X, x, nx)

    def d_recv(h, d):
        at = lax.rem(x + nx - d, nx)
        return scan_copy(3, h, d, dd.at[h, at], pd.at[h, at], X, x, nx)

    far_first = lambda n: [2, 1, 3] if n == 4 else list(range(1, n))

    def scan_a(pair):
        for h in pair:
            k = kb[:, h].reshape(2 * rows, HEAD_K)
            v = vb[:, h].reshape(2 * rows, HEAD_V)
            sa[h] = dot(k, v, ((0,), (0,))).astype(BF16).reshape(nx, chunk, HEAD_V)
        for h in pair:
            for d in far_first(nx):
                a_send(h, d).start()
        for h in pair:
            ra[h, x] = sa[h, x]

    def scan_b(h):
        for d in range(1, nx):
            a_recv(h, d).wait_recv()
        total = ra[h, 0].astype(F32)
        for i in range(1, nx):
            total += ra[h, i].astype(F32)
        tb[h] = total.astype(BF16)
        for d in far_first(ny):
            b_send(h, d).start()

        @pl.when(y == 0)
        def _():
            yp[h] = jnp.zeros(yp.shape[1:], F32)

            @pl.when(z == 0)
            def _():
                scan_back(h)

    def scan_low(h):
        @pl.when(y > 0)
        def _():
            for d in range(1, ny):

                @pl.when(y >= d)
                def _():
                    b_recv(h, d).wait_recv()
                    part = rb[h, d - 1].astype(F32)
                    yp[h] = part if d == 1 else yp[h] + part

            @pl.when(z == 0)
            def _():
                scan_back(h)

    def scan_all(h):
        for d in range(1, ny):

            @pl.when(y < d)
            def _():
                b_recv(h, d).wait_recv()

        total = tb[h].astype(F32)
        for d in range(1, ny):
            total += rb[h, d - 1].astype(F32)
        tc[h] = total.astype(BF16)
        for d in far_first(nz):

            @pl.when(z + d < nz)
            def _():
                c_send(h, d).start()

    def scan_d(h):
        @pl.when(z > 0)
        def _():
            scan_z(h)
            scan_back(h)

    def scan_z(h):
        for d in range(1, nz):

            @pl.when(z >= d)
            def _():
                c_recv(h, d).wait_recv()
                yp[h] += rc[h, d - 1].astype(F32)

    def scan_back(h):
        before = yp[h]
        for i in range(nx):
            dd[h, i] = before.astype(BF16)
            before += ra[h, i].astype(F32)
        for d in far_first(nx):
            d_send(h, d).start()
        pd[h, x] = dd[h, x]

    def scan_end(h):
        for d in range(1, nx):
            d_recv(h, d).wait_recv()

    def keys(b):
        k = dot(xn[b], wkb[...]) * jnp.exp(-level(b))
        for h in range(heads):
            kb[b, h] = k[:, h * HEAD_K : (h + 1) * HEAD_K].astype(BF16)

    def values(b, p):
        v = dot(xn[b], wvb[p]).astype(BF16)
        for i in range(2):
            vb[b, 2 * p + i] = v[:, i * HEAD_V : (i + 1) * HEAD_V]

    for s in wk_copy:
        s.wait()
    keys(c)
    for s in wv_copy[0]:
        s.wait()
    for h in range(heads):
        wo_copy(h).start(priority=1)
    values(c, 0)
    wq_copy.start(priority=1)
    for s in wg_copy:
        s.start(priority=1)
    for i in range(token_steps):
        x_recv(i).wait_recv()
    keys(other)
    values(other, 0)
    later_are_in(0)
    scan_a((0, 1))
    for s in wv_copy[1]:
        s.wait()
    wo_copy(0).wait()
    wo_send(0).start()
    values(c, 1)
    values(other, 1)
    scan_a((2, 3))

    def queries(b):
        q = dot(xn[b], wqb[...]) * (jnp.exp(level(b)) * HEAD_K**-0.5)
        for h in range(heads):
            qb[b, h] = q[:, h * HEAD_K : (h + 1) * HEAD_K].astype(BF16)

    def gates(b, p):
        u = dot(xn[b], wgb[p])
        u = u / (1.0 + jnp.exp(-u)) * hgainb[:, p * v2 : (p + 1) * v2]
        for i in range(2):
            gsb[b, 2 * p + i] = u[:, i * HEAD_V : (i + 1) * HEAD_V].astype(BF16)

    def local(h):
        i = lax.broadcasted_iota(jnp.int32, (rows, rows), 0)
        j = lax.broadcasted_iota(jnp.int32, (rows, rows), 1)
        for b in range(2):
            scores = dot(qb[b, h], kb[b, h], ((1,), (1,)))
            scores = jnp.where(i >= j, scores, 0.0).astype(BF16)
            o = dot(scores, vb[b, h])
            if b:
                scores = dot(qb[b, h], kb[0, h], ((1,), (1,))).astype(BF16)
                o += dot(scores, vb[0, h])
            lob[b, h] = o.astype(BF16)

    wq_copy.wait()
    queries(0)
    later_are_in(1)
    scan_b(0)
    wo_copy(1).wait()
    wo_send(1).start()
    queries(1)
    scan_b(1)
    for s in wg_copy:
        s.wait()
    gates(0, 0)
    scan_b(2)
    scan_b(3)
    wo_copy(2).wait()
    wo_send(2).start()
    gates(1, 0)
    scan_low(0)
    scan_low(1)
    later_are_in(2)

    @pl.when(y > 0)
    def _():
        scan_all(0)
        scan_all(1)

    gates(0, 1)

    @pl.when(y == 0)
    def _():
        scan_all(0)
        scan_all(1)

    local(0)
    scan_low(2)
    scan_low(3)

    @pl.when(y > 0)
    def _():
        scan_all(2)
        scan_all(3)


    @pl.when(y > 0)
    def _():
        scan_d(0)
        scan_d(1)

    local(1)

    @pl.when((y == 0) & (c == 0))
    def _():
        scan_all(2)
        scan_all(3)

    @pl.when(y == 0)
    def _():
        scan_d(0)
        scan_d(1)


    @pl.when((y == 0) & (c == 1))
    def _():
        scan_all(2)
        scan_all(3)

    wo_copy(3).wait()
    wo_send(3).start()
    gates(1, 1)
    scan_d(2)
    scan_d(3)

    def g_send(h):
        return remote(gsnd.at[h], gpart(h, 1), gs_s.at[h], gs_r.at[h], {TP: other})

    def carried(pair):
        for own in (False, True):
            for h in pair:
                b = c if own else other
                start = pd[h].reshape(HEAD_K, HEAD_V)
                o = lob[b, h].astype(F32) + dot(qb[b, h], start)
                scale = lax.rsqrt(jnp.mean(o * o, axis=-1, keepdims=True) + EPS)
                gated = (o * scale * gsb[b, h].astype(F32)).astype(BF16)
                if own:
                    gpart(h, 0)[...] = gated
                else:
                    gsnd[h] = gated
        for h in pair:
            g_send(h).start()

    def project(i):
        gated = jnp.concatenate([gfirst[i, 0], gfirst[i, 1]], axis=1)
        for n in range(model // UNIT):
            at = slice(n * UNIT, (n + 1) * UNIT)
            part = dot(gated, wfirst[i, :, :, at].reshape(2 * HEAD_V, UNIT))
            acc[:, at] = acc[:, at] + part if i else part

    def arrived(h):
        g_send(h).wait_recv()
        wo_send(h).wait_recv()

    local(2)
    local(3)
    scan_end(0)
    scan_end(1)
    carried((0, 1))
    project(0)
    scan_end(2)
    scan_end(3)
    carried((2, 3))
    arrived(0)
    arrived(1)
    project(1)
    for h in range(2, heads):
        arrived(h)

    for i in range(token_steps):
        x_send(i).wait_send()
    for h in range(heads):
        wo_send(h).wait_send()
        g_send(h).wait_send()
        for d in range(1, nx):
            a_send(h, d).wait_send()
            d_send(h, d).wait_send()
        for d in range(1, ny):
            b_send(h, d).wait_send()
        for d in range(1, nz):

            @pl.when(z + d < nz)
            def _():
                c_send(h, d).wait_send()


def finish(acc, gated, weight, out, stage, sem):
    rows, model = acc.shape
    depth = weight.shape[0] * 2 * HEAD_V
    left = jnp.concatenate([gated[h, i] for h in range(weight.shape[0]) for i in range(2)], axis=1)
    copies = []
    for n in range(model // UNIT):
        at = slice(n * UNIT, (n + 1) * UNIT)
        right = weight[:, :, :, at].reshape(depth, UNIT)
        stage[n] = (acc[:, at] + dot(left, right)).astype(BF16)
        copies.append(pltpu.make_async_copy(stage.at[n], out.at[:, pl.ds(n * UNIT, UNIT)], sem.at[n]))
        if n:
            copies[n - 1].start()
    copies[-1].start()
    for copy in copies:
        copy.wait()


def on_device(sizes, tok, gain, wq, wk, wv, wg, bias, hgain, wo):
    nz, ny, nx = sizes
    rows, width = tok.shape
    key_width, value_width, model = wq.shape[1], wv.shape[1], wo.shape[1]
    heads = key_width // HEAD_K
    pairs = heads // 2
    token_steps = 4
    most = max(sizes) - 1
    vmem = pltpu.VMEM
    dma = pltpu.SemaphoreType.DMA
    quarter = (HEAD_K // nx, HEAD_V)
    scratch = [
        vmem((2, rows, width), BF16),
        vmem((width, key_width), BF16),
        vmem((pairs, width, 2 * HEAD_V), BF16),
        vmem((width, key_width), BF16),
        vmem((pairs, width, 2 * HEAD_V), BF16),
        vmem((2, 2, HEAD_V, model), BF16),
        vmem((1, width), F32),
        vmem((1, key_width), F32),
        vmem((1, value_width), F32),
        vmem((2, heads, rows, HEAD_K), BF16),
        vmem((2, heads, rows, HEAD_K), BF16),
        vmem((2, heads, rows, HEAD_V), BF16),
        vmem((2, heads, rows, HEAD_V), BF16),
        vmem((2, heads, rows, HEAD_V), BF16),
        vmem((heads, nx, *quarter), BF16),
        vmem((heads, nx, *quarter), BF16),
        vmem((heads, *quarter), BF16),
        vmem((heads, ny - 1, *quarter), BF16),
        vmem((heads, *quarter), F32),
        vmem((heads, *quarter), BF16),
        vmem((heads, nz - 1, *quarter), BF16),
        vmem((heads, nx, *quarter), BF16),
        vmem((heads, nx, *quarter), BF16),
        vmem((2, 2, rows, HEAD_V), BF16),
        vmem((heads, rows, HEAD_V), BF16),
        dma((token_steps,)),
        dma((3,)),
        dma((4,)),
        dma((pairs, 4)),
        dma((1,)),
        dma((pairs,)),
        dma((heads,)),
        dma((token_steps,)),
        dma((token_steps,)),
        dma((heads,)),
        dma((heads,)),
        dma((heads,)),
        dma((heads,)),
        dma((4, heads, most)),
        dma((4, heads, most)),
        pltpu.SemaphoreType.REGULAR((3,)),
    ]
    hbm = pl.BlockSpec(memory_space=pl.ANY)
    in_vmem = pl.BlockSpec(memory_space=vmem)
    parts = pl.pallas_call(
        functools.partial(mixer, sizes),
        out_shape=(
            vmem((rows, model), F32),
            vmem((heads - 2, 2, rows, HEAD_V), BF16),
            vmem((heads - 2, 2, HEAD_V, model), BF16),
        ),
        in_specs=[hbm] * 9,
        out_specs=[in_vmem] * 3,
        scratch_shapes=scratch,
        compiler_params=pltpu.CompilerParams(
            collective_id=0, has_side_effects=True, vmem_limit_bytes=52_500_000
        ),
        name="mixer",
    )(
        tok, gain.reshape(1, -1), wq, wk, wv, wg, bias.reshape(1, -1), hgain.reshape(1, -1), wo
    )
    return pl.pallas_call(
        finish,
        out_shape=jax.ShapeDtypeStruct((rows, model), BF16),
        in_specs=[in_vmem] * 3,
        out_specs=hbm,
        scratch_shapes=[vmem((model // UNIT, rows, UNIT), BF16), dma((model // UNIT,))],
        compiler_params=pltpu.CompilerParams(vmem_limit_bytes=8_000_000),
        name="finish",
    )(*parts)


def solution(mesh, sizes=(4, 4, 4)):
    finer = Mesh(mesh.devices.reshape(*sizes, mesh.shape["tp"]), SP_TP)
    in_specs = (
        P(SP_TP, None),
        P(),
        P(None, "tp"),
        P(None, "tp"),
        P(None, "tp"),
        P(None, "tp"),
        P("tp"),
        P("tp"),
        P("tp", None),
    )
    return jax.shard_map(
        functools.partial(on_device, sizes),
        mesh=finer,
        in_specs=in_specs,
        out_specs=P(SP_TP, None),
        check_vma=False,
    )
```

```python
import functools
import math

import jax
import jax.numpy as jnp
from jax import lax
from jax.experimental import pallas as pl
from jax.experimental.pallas import tpu as pltpu
from jax.sharding import Mesh
from jax.sharding import PartitionSpec as P

HEAD_K = 128
HEAD_V = 256
Z, Y, X, TP = "sp_0", "sp_1", "sp_2", "tp"
SP_TP = (Z, Y, X, TP)
MESH = pl.DeviceIdType.MESH
UNIT = 512
EPS = 1e-06
DECAY_POWER = 16.0
F32, BF16 = jnp.float32, jnp.bfloat16


def remote(src, dst, send, recv, where):
    return pltpu.make_async_remote_copy(
        src_ref=src, dst_ref=dst, send_sem=send, recv_sem=recv, device_id=where, device_id_type=MESH
    )


def dot(a, b, dims=((1,), (0,))):
    return lax.dot_general(a, b, (dims, ((), ())), preferred_element_type=F32)


def mixer(
    sizes,
    tok, gain, wq, wk, wv, wg, bias, hgain, wo,
    acc, gall, wob,
    xn, wkb, wvb, wqb, wgb, wfirst, gainb, biasb, hgainb,
    kb, qb, vb, gsb, lob,
    sa, ra, tb, rb, yp, tc, rc, dd, pd,
    gfirst, gsnd,
    tok_sem, small_sem, k_sem, v_sem, q_sem, g_sem, wo_sem,
    xs, xr, ps, pr, gs_s, gs_r, scan_s, scan_r, line_sem,
):
    nz, ny, nx = sizes
    rows, width = xn.shape[1], xn.shape[2]
    heads = kb.shape[1]
    pairs = heads // 2
    chunk = HEAD_K // nx
    token_steps = tok_sem.shape[0]
    step_rows = rows // token_steps
    model = acc.shape[1]
    wpart = lambda h, i: wob.at[h - 2, i] if h > 1 else wfirst.at[i, h]
    gpart = lambda h, i: gall.at[h - 2, i] if h > 1 else gfirst.at[i, h]
    z, y, x, c = (lax.axis_index(a) for a in SP_TP)
    other = 1 - c
    chip = (z * ny + y) * nx + x
    seq = nz * ny * nx * 2 * rows

    def token_copy(i):
        r = pl.ds(i * step_rows, step_rows)
        return pltpu.make_async_copy(tok.at[r, :], xn.at[c, r, :], tok_sem.at[i])

    small = [(gain, gainb), (bias, biasb), (hgain, hgainb)]
    small = [pltpu.make_async_copy(a, b, small_sem.at[i]) for i, (a, b) in enumerate(small)]
    v2 = 2 * HEAD_V
    wk_copy = pltpu.make_async_copy(wk, wkb, k_sem.at[0])
    wv_copy = [pltpu.make_async_copy(wv.at[:, pl.ds(p * v2, v2)], wvb.at[p], v_sem.at[p]) for p in range(pairs)]
    wq_copy = pltpu.make_async_copy(wq, wqb, q_sem.at[0])
    wg_copy = [pltpu.make_async_copy(wg.at[:, pl.ds(p * v2, v2)], wgb.at[p], g_sem.at[p]) for p in range(pairs)]

    def wo_copy(h):
        return pltpu.make_async_copy(wo.at[pl.ds(h * HEAD_V, HEAD_V), :], wpart(h, 0), wo_sem.at[h])

    def wo_send(h):
        return remote(wpart(h, 0), wpart(h, 1), ps.at[h], pr.at[h], {TP: other})

    for s in small:
        s.start()
    for i in range(token_steps):
        token_copy(i).start()
    wk_copy.start(priority=1)

    barrier = pltpu.get_barrier_semaphore()
    lines = [(X, x, nx), (Y, y, ny), (Z, z, nz)]
    pl.semaphore_signal(barrier, inc=1, device_id={TP: other}, device_id_type=MESH)
    for axis, at, n in lines:
        for d in range(1, n):

            @pl.when(at + d < n)
            def _():
                pl.semaphore_signal(barrier, inc=1, device_id={axis: lax.rem(at + d, n)}, device_id_type=MESH)

    def tell_earlier():
        for i, (axis, at, n) in enumerate(lines):
            for d in range(1, n):

                @pl.when(at >= d)
                def _():
                    to = {axis: lax.rem(at - d + n, n)}
                    pl.semaphore_signal(line_sem.at[i], inc=1, device_id=to, device_id_type=MESH)

    def later_are_in(i):
        _, at, n = lines[i]

        @pl.when(at + 1 < n)
        def _():
            pl.semaphore_wait(line_sem.at[i], n - 1 - at)

    def x_send(i):
        r = pl.ds(i * step_rows, step_rows)
        return remote(xn.at[c, r, :], xn.at[c, r, :], xs.at[i], xr.at[i], {TP: other})

    def x_recv(i):
        r = pl.ds(i * step_rows, step_rows)
        return remote(xn.at[other, r, :], xn.at[other, r, :], xs.at[i], xr.at[i], {TP: other})

    for s in small:
        s.wait()
    for i in range(token_steps):
        token_copy(i).wait()
        if i == 0:
            wv_copy[0].start(priority=1)
        if i == token_steps - 1:
            wv_copy[1].start(priority=1)

        for g in range(step_rows // 16):
            r = pl.ds(i * step_rows + g * 16, 16)
            v = xn[c, r, :].astype(F32)
            scale = lax.rsqrt(jnp.mean(v * v, axis=-1, keepdims=True) + EPS)
            v = xn[c, r, :].astype(F32)
            xn[c, r, :] = (v * scale * gainb[...]).astype(BF16)
        if i == 0:
            pl.semaphore_wait(barrier, 1 + x + y + z)
        x_send(i).start()


    tell_earlier()

    logits = biasb[...] + math.log(seq / 8.0)
    log_decay = (jnp.minimum(logits, 0.0) - jnp.log1p(jnp.exp(-jnp.abs(logits)))) / DECAY_POWER

    def level(b):
        row = lax.broadcasted_iota(jnp.int32, (rows, 1), 0)
        pos = (row + (chip * 2 + b) * rows + (1 - seq // 2)).astype(F32)
        return pos * log_decay

    def scan_copy(phase, h, d, src, dst, axis, at, n):
        to = lax.rem(at + d, n)
        return remote(src, dst, scan_s.at[phase, h, d - 1], scan_r.at[phase, h, d - 1], {axis: to})

    def a_send(h, d):
        return scan_copy(0, h, d, sa.at[h, lax.rem(x + d, nx)], ra.at[h, x], X, x, nx)

    def a_recv(h, d):
        at = lax.rem(x + nx - d, nx)
        return scan_copy(0, h, d, sa.at[h, at], ra.at[h, at], X, x, nx)

    def b_send(h, d):
        return scan_copy(1, h, d, tb.at[h], rb.at[h, d - 1], Y, y, ny)

    def b_recv(h, d):
        return scan_copy(1, h, d, tb.at[h], rb.at[h, d - 1], Y, y, ny)

    def c_send(h, d):
        return scan_copy(2, h, d, tc.at[h], rc.at[h, d - 1], Z, z, nz)

    def c_recv(h, d):
        return scan_copy(2, h, d, tc.at[h], rc.at[h, d - 1], Z, z, nz)

    def d_send(h, d):
        return scan_copy(3, h, d, dd.at[h, lax.rem(x + d, nx)], pd.at[h, x], X, x, nx)

    def d_recv(h, d):
        at = lax.rem(x + nx - d, nx)
        return scan_copy(3, h, d, dd.at[h, at], pd.at[h, at], X, x, nx)

    far_first = lambda n: [2, 1, 3] if n == 4 else list(range(1, n))

    def scan_a(pair):
        for h in pair:
            k = kb[:, h].reshape(2 * rows, HEAD_K)
            v = vb[:, h].reshape(2 * rows, HEAD_V)
            sa[h] = dot(k, v, ((0,), (0,))).astype(BF16).reshape(nx, chunk, HEAD_V)
        for h in pair:
            for d in far_first(nx):
                a_send(h, d).start()
        for h in pair:
            ra[h, x] = sa[h, x]

    def scan_b(h):
        for d in range(1, nx):
            a_recv(h, d).wait_recv()
        total = ra[h, 0].astype(F32)
        for i in range(1, nx):
            total += ra[h, i].astype(F32)
        tb[h] = total.astype(BF16)
        for d in far_first(ny):
            b_send(h, d).start()

        @pl.when(y == 0)
        def _():
            yp[h] = jnp.zeros(yp.shape[1:], F32)

            @pl.when(z == 0)
            def _():
                scan_back(h)

    def scan_low(h):
        @pl.when(y > 0)
        def _():
            for d in range(1, ny):

                @pl.when(y >= d)
                def _():
                    b_recv(h, d).wait_recv()
                    part = rb[h, d - 1].astype(F32)
                    yp[h] = part if d == 1 else yp[h] + part

            @pl.when(z == 0)
            def _():
                scan_back(h)

    def scan_all(h):
        for d in range(1, ny):

            @pl.when(y < d)
            def _():
                b_recv(h, d).wait_recv()

        total = tb[h].astype(F32)
        for d in range(1, ny):
            total += rb[h, d - 1].astype(F32)
        tc[h] = total.astype(BF16)
        for d in far_first(nz):

            @pl.when(z + d < nz)
            def _():
                c_send(h, d).start()

    def scan_d(h):
        @pl.when(z > 0)
        def _():
            scan_z(h)
            scan_back(h)

    def scan_z(h):
        for d in range(1, nz):

            @pl.when(z >= d)
            def _():
                c_recv(h, d).wait_recv()
                yp[h] += rc[h, d - 1].astype(F32)

    def scan_back(h):
        before = yp[h]
        for i in range(nx):
            dd[h, i] = before.astype(BF16)
            before += ra[h, i].astype(F32)
        for d in far_first(nx):
            d_send(h, d).start()
        pd[h, x] = dd[h, x]

    def scan_end(h):
        for d in range(1, nx):
            d_recv(h, d).wait_recv()

    def keys(b):
        k = dot(xn[b], wkb[...]) * jnp.exp(-level(b))
        for h in range(heads):
            kb[b, h] = k[:, h * HEAD_K : (h + 1) * HEAD_K].astype(BF16)

    def values(b, p):
        v = dot(xn[b], wvb[p]).astype(BF16)
        for i in range(2):
            vb[b, 2 * p + i] = v[:, i * HEAD_V : (i + 1) * HEAD_V]

    wk_copy.wait()
    keys(c)
    wv_copy[0].wait()
    for h in range(heads):
        wo_copy(h).start(priority=1)
    values(c, 0)
    wq_copy.start(priority=1)
    for s in wg_copy:
        s.start(priority=1)
    for i in range(token_steps):
        x_recv(i).wait_recv()
    keys(other)
    values(other, 0)
    later_are_in(0)
    scan_a((0, 1))
    wv_copy[1].wait()
    wo_copy(0).wait()
    wo_send(0).start()
    values(c, 1)
    values(other, 1)
    scan_a((2, 3))

    def queries(b):
        q = dot(xn[b], wqb[...]) * (jnp.exp(level(b)) * HEAD_K**-0.5)
        for h in range(heads):
            qb[b, h] = q[:, h * HEAD_K : (h + 1) * HEAD_K].astype(BF16)

    def gates(b, p):
        u = dot(xn[b], wgb[p])
        u = u / (1.0 + jnp.exp(-u)) * hgainb[:, p * v2 : (p + 1) * v2]
        for i in range(2):
            gsb[b, 2 * p + i] = u[:, i * HEAD_V : (i + 1) * HEAD_V].astype(BF16)

    def local(h):
        i = lax.broadcasted_iota(jnp.int32, (rows, rows), 0)
        j = lax.broadcasted_iota(jnp.int32, (rows, rows), 1)
        for b in range(2):
            scores = dot(qb[b, h], kb[b, h], ((1,), (1,)))
            scores = jnp.where(i >= j, scores, 0.0).astype(BF16)
            o = dot(scores, vb[b, h])
            if b:
                scores = dot(qb[b, h], kb[0, h], ((1,), (1,))).astype(BF16)
                o += dot(scores, vb[0, h])
            lob[b, h] = o.astype(BF16)

    wq_copy.wait()
    queries(0)
    later_are_in(1)
    scan_b(0)
    wo_copy(1).wait()
    wo_send(1).start()
    queries(1)
    scan_b(1)
    for s in wg_copy:
        s.wait()
    gates(0, 0)
    scan_b(2)
    scan_b(3)
    wo_copy(2).wait()
    wo_send(2).start()
    gates(1, 0)
    scan_low(0)
    scan_low(1)
    later_are_in(2)

    @pl.when(y > 0)
    def _():
        scan_all(0)
        scan_all(1)

    gates(0, 1)

    @pl.when(y == 0)
    def _():
        scan_all(0)
        scan_all(1)

    local(0)
    scan_low(2)
    scan_low(3)

    @pl.when(y > 0)
    def _():
        scan_all(2)
        scan_all(3)


    @pl.when(y > 0)
    def _():
        scan_d(0)
        scan_d(1)

    local(1)

    @pl.when((y == 0) & (c == 0))
    def _():
        scan_all(2)
        scan_all(3)

    @pl.when(y == 0)
    def _():
        scan_d(0)
        scan_d(1)


    @pl.when((y == 0) & (c == 1))
    def _():
        scan_all(2)
        scan_all(3)

    wo_copy(3).wait()
    wo_send(3).start()
    gates(1, 1)
    scan_d(2)
    scan_d(3)

    def g_send(h):
        return remote(gsnd.at[h], gpart(h, 1), gs_s.at[h], gs_r.at[h], {TP: other})

    def carried(pair):
        for own in (False, True):
            for h in pair:
                b = c if own else other
                start = pd[h].reshape(HEAD_K, HEAD_V)
                o = lob[b, h].astype(F32) + dot(qb[b, h], start)
                scale = lax.rsqrt(jnp.mean(o * o, axis=-1, keepdims=True) + EPS)
                gated = (o * scale * gsb[b, h].astype(F32)).astype(BF16)
                if own:
                    gpart(h, 0)[...] = gated
                else:
                    gsnd[h] = gated
        for h in pair:
            g_send(h).start()

    def project(i):
        gated = jnp.concatenate([gfirst[i, 0], gfirst[i, 1]], axis=1)
        for n in range(model // UNIT):
            at = slice(n * UNIT, (n + 1) * UNIT)
            part = dot(gated, wfirst[i, :, :, at].reshape(2 * HEAD_V, UNIT))
            acc[:, at] = acc[:, at] + part if i else part

    def arrived(h):
        g_send(h).wait_recv()
        wo_send(h).wait_recv()

    local(2)
    local(3)
    scan_end(0)
    scan_end(1)
    carried((0, 1))
    project(0)
    scan_end(2)
    scan_end(3)
    carried((2, 3))
    arrived(0)
    arrived(1)
    project(1)
    for h in range(2, heads):
        arrived(h)

    for i in range(token_steps):
        x_send(i).wait_send()
    for h in range(heads):
        wo_send(h).wait_send()
        g_send(h).wait_send()
        for d in range(1, nx):
            a_send(h, d).wait_send()
            d_send(h, d).wait_send()
        for d in range(1, ny):
            b_send(h, d).wait_send()
        for d in range(1, nz):

            @pl.when(z + d < nz)
            def _():
                c_send(h, d).wait_send()


def finish(acc, gated, weight, out, stage, sem):
    rows, model = acc.shape
    depth = weight.shape[0] * 2 * HEAD_V
    left = jnp.concatenate([gated[h, i] for h in range(weight.shape[0]) for i in range(2)], axis=1)
    copies = []
    for n in range(model // UNIT):
        at = slice(n * UNIT, (n + 1) * UNIT)
        right = weight[:, :, :, at].reshape(depth, UNIT)
        stage[n] = (acc[:, at] + dot(left, right)).astype(BF16)
        copies.append(pltpu.make_async_copy(stage.at[n], out.at[:, pl.ds(n * UNIT, UNIT)], sem.at[n]))
        if n:
            copies[n - 1].start()
    copies[-1].start()
    for copy in copies:
        copy.wait()


def on_device(sizes, tok, gain, wq, wk, wv, wg, bias, hgain, wo):
    nz, ny, nx = sizes
    rows, width = tok.shape
    key_width, value_width, model = wq.shape[1], wv.shape[1], wo.shape[1]
    heads = key_width // HEAD_K
    pairs = heads // 2
    token_steps = 4
    most = max(sizes) - 1
    vmem = pltpu.VMEM
    dma = pltpu.SemaphoreType.DMA
    quarter = (HEAD_K // nx, HEAD_V)
    scratch = [
        vmem((2, rows, width), BF16),
        vmem((width, key_width), BF16),
        vmem((pairs, width, 2 * HEAD_V), BF16),
        vmem((width, key_width), BF16),
        vmem((pairs, width, 2 * HEAD_V), BF16),
        vmem((2, 2, HEAD_V, model), BF16),
        vmem((1, width), F32),
        vmem((1, key_width), F32),
        vmem((1, value_width), F32),
        vmem((2, heads, rows, HEAD_K), BF16),
        vmem((2, heads, rows, HEAD_K), BF16),
        vmem((2, heads, rows, HEAD_V), BF16),
        vmem((2, heads, rows, HEAD_V), BF16),
        vmem((2, heads, rows, HEAD_V), BF16),
        vmem((heads, nx, *quarter), BF16),
        vmem((heads, nx, *quarter), BF16),
        vmem((heads, *quarter), BF16),
        vmem((heads, ny - 1, *quarter), BF16),
        vmem((heads, *quarter), F32),
        vmem((heads, *quarter), BF16),
        vmem((heads, nz - 1, *quarter), BF16),
        vmem((heads, nx, *quarter), BF16),
        vmem((heads, nx, *quarter), BF16),
        vmem((2, 2, rows, HEAD_V), BF16),
        vmem((heads, rows, HEAD_V), BF16),
        dma((token_steps,)),
        dma((3,)),
        dma((1,)),
        dma((pairs,)),
        dma((1,)),
        dma((pairs,)),
        dma((heads,)),
        dma((token_steps,)),
        dma((token_steps,)),
        dma((heads,)),
        dma((heads,)),
        dma((heads,)),
        dma((heads,)),
        dma((4, heads, most)),
        dma((4, heads, most)),
        pltpu.SemaphoreType.REGULAR((3,)),
    ]
    hbm = pl.BlockSpec(memory_space=pl.ANY)
    in_vmem = pl.BlockSpec(memory_space=vmem)
    parts = pl.pallas_call(
        functools.partial(mixer, sizes),
        out_shape=(
            vmem((rows, model), F32),
            vmem((heads - 2, 2, rows, HEAD_V), BF16),
            vmem((heads - 2, 2, HEAD_V, model), BF16),
        ),
        in_specs=[hbm] * 9,
        out_specs=[in_vmem] * 3,
        scratch_shapes=scratch,
        compiler_params=pltpu.CompilerParams(
            collective_id=0, has_side_effects=True, vmem_limit_bytes=52_500_000
        ),
        name="mixer",
    )(
        tok, gain.reshape(1, -1), wq, wk, wv, wg, bias.reshape(1, -1), hgain.reshape(1, -1), wo
    )
    return pl.pallas_call(
        finish,
        out_shape=jax.ShapeDtypeStruct((rows, model), BF16),
        in_specs=[in_vmem] * 3,
        out_specs=hbm,
        scratch_shapes=[vmem((model // UNIT, rows, UNIT), BF16), dma((model // UNIT,))],
        compiler_params=pltpu.CompilerParams(vmem_limit_bytes=8_000_000),
        name="finish",
    )(*parts)


def solution(mesh, sizes=(4, 4, 4)):
    finer = Mesh(mesh.devices.reshape(*sizes, mesh.shape["tp"]), SP_TP)
    in_specs = (
        P(SP_TP, None),
        P(),
        P(None, "tp"),
        P(None, "tp"),
        P(None, "tp"),
        P(None, "tp"),
        P("tp"),
        P("tp"),
        P("tp", None),
    )
    return jax.shard_map(
        functools.partial(on_device, sizes),
        mesh=finer,
        in_specs=in_specs,
        out_specs=P(SP_TP, None),
        check_vma=False,
    )
```
